128 devices in a mesh: sp: 32 (over z, y, core), tp: 4 (over x).
Axes of the slice: x: 4, y: 4, z: 4, core: 2. Of those that a mesh axis runs over, the one named last changes fastest.
Arguments:
- tokens: bfloat16 [12288, 2048], P(('sp', 'tp')), may hold values from -8 to 8, as said below
- query_weight: bfloat16 [2048, 1024], P(None, 'tp'), as said below
- key_weight: bfloat16 [2048, 256], P(None, 'tp'), as said below
- value_weight: bfloat16 [2048, 256], P(None, 'tp'), may hold values from -0.125 to 0.125
- out_weight: bfloat16 [1024, 2048], P('tp'), may hold values from -0.75 to 0.75
- query_gain: bfloat16 [16, 64], P('tp'), may hold values from 0.5 to 6.5
- key_gain: bfloat16 [4, 64], P('tp'), may hold values from 0.5 to 6.5
Outputs:
- mixed: bfloat16 [12288, 2048], P(('sp', 'tp'))
- log_sums: float32 [16, 12288], P('tp', 'sp')
The draws below stay inside these ranges and needn't reach their ends.
Inputs may be any that keep to these rules, and one draw needn't show every extreme that they name: Each block of 384 consecutive tokens has a mean vector of its own. `query_weight`: entries are those of a weight over 2048 inputs, of magnitude at most 6 / sqrt(2048). `key_weight`: entries are those of a weight over 2048 inputs, of magnitude at most 6 / sqrt(2048).
All inputs are finite; a program needn't handle non-finite values.
Results may differ from the reference program's by a relative error of at most 0.028.
Values may be sent and summed in bfloat16 or wider, within the bound.
A program may use at most 64 MiB of HBM per device.

```python
import math
import jax
import jax.numpy as jnp
from jax import lax

D = 2048
HEADS = 16
KV_HEADS = 4
HD = 64
GRID_W = 64
TOK_DEV = 384
TOKENS = 12288
N_TP = 4


def shared_query(key):
    base = jnp.clip(jax.random.normal(jax.random.fold_in(key, 11), (D, HEADS * HD), jnp.float32), -6.0, 6.0)
    base = base * D ** (-0.5)
    return base


def draw_tokens(key, part):
    offsets = jax.random.normal(jax.random.fold_in(key, 21), (TOKENS // TOK_DEV, D), jnp.float32)
    offsets = jnp.repeat(offsets, TOK_DEV, axis=0)
    noise = jax.random.normal(jax.random.fold_in(key, 22), (TOKENS, D), jnp.float32)
    return jnp.clip(noise + offsets, -8.0, 8.0).astype(jnp.bfloat16)


def draw_query_weight(key, part):
    return shared_query(key).astype(jnp.bfloat16)


def draw_key_weight(key, part):
    base = jnp.clip(jax.random.normal(jax.random.fold_in(key, 12), (D, KV_HEADS * HD), jnp.float32), -6.0, 6.0)
    return (base * D ** (-0.5)).astype(jnp.bfloat16)


def draw_query_gain(key, part):
    usual = jax.random.uniform(jax.random.fold_in(key, 31), (HEADS, HD), jnp.float32, 0.5, 1.5)
    return usual.astype(jnp.bfloat16)


def draw_key_gain(key, part):
    return jax.random.uniform(jax.random.fold_in(key, 41), (KV_HEADS, HD), jnp.float32, 0.5, 1.5).astype(jnp.bfloat16)


def level_of(key, shape, shards, low, largest):
    loudness = 1.0
    for dim, blocks in shards:
        draws = jax.random.uniform(jax.random.fold_in(jax.random.fold_in(key, 6), dim), (blocks,), jnp.float32, low / len(shards), largest / len(shards))
        loudness = loudness * jnp.repeat(jnp.exp(draws), shape[dim] // blocks).reshape((-1,) + (1,) * (len(shape) - 1 - dim))
    return loudness


def bell_draw(stream_key, dims, scale, reach, shards=(), held_as=jnp.bfloat16):
    loudness = level_of(stream_key, dims, shards, -0.22, 0.18) if shards else 1.0
    drawn = jax.random.normal(stream_key, dims, jnp.float32) * scale * loudness
    return jnp.minimum(jnp.maximum(drawn, -reach), reach).astype(held_as)


def setup_inputs(seed: int = 0) -> dict:
    key_of = jax.random.split(jax.random.key(seed), 8)
    return {
        "tokens": draw_tokens(jax.random.fold_in(key_of[7], 71), 0),
        "query_weight": draw_query_weight(jax.random.fold_in(key_of[7], 71), 0),
        "key_weight": draw_key_weight(jax.random.fold_in(key_of[7], 71), 0),
        "value_weight": bell_draw(key_of[3], (D, KV_HEADS * HD), D ** -0.5, 0.125, ((1, 4),)),
        "out_weight": bell_draw(key_of[4], (HEADS * HD, D), (HEADS * HD // 16) ** -0.5, 0.75, ((0, 4),)),
        "query_gain": draw_query_gain(jax.random.fold_in(key_of[7], 71), 0),
        "key_gain": draw_key_gain(jax.random.fold_in(key_of[7], 71), 0),
    }


def angle_tables(count):
    quarter = HD // 4
    place = jnp.arange(count, dtype=jnp.int32)
    grid_row = (place // GRID_W).astype(jnp.float32)
    grid_col = (place % GRID_W).astype(jnp.float32)
    freq = 10000.0 ** (-jnp.arange(quarter, dtype=jnp.float32).astype(jnp.float32) / quarter)
    row_angle = grid_row[:, None] * freq[None, :]
    col_angle = grid_col[:, None] * freq[None, :]
    return (jnp.cos(row_angle), jnp.sin(row_angle), jnp.cos(col_angle), jnp.sin(col_angle))

def turn_pairs(part, cosine, sine):
    quarter = part.shape[-1] // 2
    first = part[..., :quarter]
    second = part[..., quarter:]
    cosine = cosine[:, None, :]
    sine = sine[:, None, :]
    return jnp.concatenate([first * cosine - second * sine, second * cosine + first * sine], axis=-1)

def prepare(raw, gain, tables):
    count = raw.shape[0]
    heads = gain.shape[0]
    values = raw.astype(jnp.float32).reshape(count, heads, HD)
    scaled = values * lax.rsqrt(lax.optimization_barrier(jnp.mean(values * values, axis=-1, keepdims=True)) + 1e-06)
    scaled = scaled * gain.astype(jnp.float32)[None, :, :]
    half = HD // 2
    row_cos, row_sin, col_cos, col_sin = tables
    turned = jnp.concatenate([turn_pairs(scaled[..., :half], row_cos, row_sin), turn_pairs(scaled[..., half:], col_cos, col_sin)], axis=-1)
    return turned.astype(jnp.bfloat16)

def reference(tokens, query_weight, key_weight, value_weight, out_weight, query_gain, key_gain):
    count = tokens.shape[0]
    query_raw = jnp.dot(tokens, query_weight, preferred_element_type=jnp.float32).astype(jnp.bfloat16)
    key_raw = jnp.dot(tokens, key_weight, preferred_element_type=jnp.float32).astype(jnp.bfloat16)
    values = jnp.dot(tokens, value_weight, preferred_element_type=jnp.float32).astype(jnp.bfloat16)
    tables = angle_tables(count)
    queries = prepare(query_raw, query_gain, tables)
    keys = prepare(key_raw, key_gain, tables)
    share = HEADS // KV_HEADS
    key_float = keys.astype(jnp.float32)
    value_float = values.reshape(count, KV_HEADS, HD).astype(jnp.float32)
    block_len = math.gcd(count, 128)
    blocks = queries.reshape(count // block_len, block_len, KV_HEADS, share, HD)

    def one_block(query_block):
        scores = jnp.einsum('qhgd,khd->hgqk', query_block.astype(jnp.float32), key_float, precision=lax.Precision.HIGHEST) * HD ** (-0.5)
        row_max = lax.optimization_barrier(jnp.max(scores, axis=-1))
        expo = jnp.exp(scores - row_max[..., None])
        totals = lax.optimization_barrier(jnp.sum(expo, axis=-1))
        weights = lax.optimization_barrier(expo.astype(jnp.bfloat16)).astype(jnp.float32)
        summed = jnp.einsum('hgqk,khd->qhgd', weights, value_float, precision=lax.Precision.HIGHEST)
        attended = summed / jnp.transpose(totals, (2, 0, 1))[..., None]
        log_block = (row_max + jnp.log(totals)).reshape(HEADS, block_len)
        return (attended.astype(jnp.bfloat16).reshape(block_len, HEADS * HD), log_block)
    attended, log_blocks = lax.map(one_block, blocks)
    attended = attended.reshape(count, HEADS * HD)
    log_sums = jnp.transpose(log_blocks, (1, 0, 2)).reshape(HEADS, count)
    group_width = HEADS // N_TP * HD
    total = jnp.zeros((count, D), jnp.float32)
    for group in range(N_TP):
        lo = group * group_width
        partial_sum = jnp.dot(attended[:, lo:lo + group_width], out_weight[lo:lo + group_width], preferred_element_type=jnp.float32).astype(jnp.bfloat16)
        total = total + partial_sum.astype(jnp.float32)
    return (total.astype(jnp.bfloat16), log_sums)
```

```python
import functools
import math

import jax
import jax.numpy as jnp
from jax import lax
from jax.experimental import pallas as pl
from jax.experimental.pallas import tpu as pltpu
from jax.sharding import PartitionSpec as P

GRID_W = 64
ROPE_BASE = 10000.0
EPS = 1e-06
LOG2E = math.log2(math.e)
LN2 = math.log(2.0)
ONES = 16
RING = 4
CHUNK = 768
TILE = 256
SUB = 256
MESH = pl.DeviceIdType.MESH
F32 = jnp.float32
BF16 = jnp.bfloat16


def prepare(x, gain, tables):
    quarter = x.shape[0] // 4
    x = x * lax.rsqrt(jnp.mean(x * x, axis=0, keepdims=True) + EPS) * gain
    a, b, c, d = (x[i * quarter : (i + 1) * quarter] for i in range(4))
    row_cos, row_sin, col_cos, col_sin = tables
    return jnp.concatenate(
        [
            a * row_cos - b * row_sin,
            b * row_cos + a * row_sin,
            c * col_cos - d * col_sin,
            d * col_cos + c * col_sin,
        ],
        axis=0,
    )


def angle_tables(first, count, quarter):
    place = first + lax.broadcasted_iota(jnp.int32, (quarter, count), 1)
    order = lax.broadcasted_iota(jnp.int32, (quarter, count), 0).astype(F32)
    freq = jnp.exp(order * (-math.log(ROPE_BASE) / quarter))
    shift = GRID_W.bit_length() - 1
    row = lax.shift_right_logical(place, shift).astype(F32) * freq
    col = jnp.bitwise_and(place, GRID_W - 1).astype(F32) * freq
    return (jnp.cos(row), jnp.sin(row), jnp.cos(col), jnp.sin(col))


def kernel(
    tok_hbm,
    wq_hbm,
    wk_hbm,
    wv_hbm,
    wo_hbm,
    qg_ref,
    kg_ref,
    mixed_ref,
    log_ref,
    tok,
    wq,
    wkv,
    wo,
    gains,
    raw,
    queries,
    kv,
    scores,
    peak,
    turned_v,
    acc,
    top,
    att,
    att_in,
    local_sem,
    tok_send,
    tok_recv,
    kv_send,
    kv_recv,
    wo_send,
    wo_recv,
    att_send,
    att_recv,
):
    sp = lax.axis_index("sp")
    tp = lax.axis_index("tp")
    core = lax.rem(sp, 2)
    y = lax.rem(sp // 2, RING)
    z = sp // (2 * RING)
    mate = sp + 1 - 2 * core
    left, right, opposite = (lax.rem(tp + i, RING) for i in (3, 1, 2))
    n_sp = RING * RING * 2
    rows = tok.shape[1]
    half = rows // 2
    heads, width = qg_ref.shape
    count = rows * RING
    query_cols = wq.shape[1]
    kv_cols = wk_hbm.shape[0]
    group = wo_hbm.shape[0]
    n_tiles = heads * count // TILE
    n_chunks = n_sp * count // CHUNK

    coord_a = y * (1 - core) + z * core
    step_a = 2 + 6 * core
    coord_b = z * (1 - core) + y * core
    step_b = 8 - 6 * core

    def shift_a(i):
        return (lax.rem(coord_a + i, RING) - coord_a) * step_a

    def shift_b(i):
        return (lax.rem(coord_b + i, RING) - coord_b) * step_b

    loads = [
        pltpu.make_async_copy(src, dst, local_sem.at[i])
        for i, (src, dst) in enumerate(
            (
                (tok_hbm, tok.at[tp]),
                (wq_hbm, wq),
                (wk_hbm, wkv.at[0:kv_cols]),
                (wv_hbm, wkv.at[kv_cols:]),
                (wo_hbm, wo.at[tp]),
            )
        )
    ]
    for load in loads:
        load.start()

    barrier = pltpu.get_barrier_semaphore()
    for i in range(1, RING):
        pl.semaphore_signal(barrier, inc=1, device_id={"tp": lax.rem(tp + i, RING)}, device_id_type=MESH)
        pl.semaphore_signal(barrier, inc=1, device_id={"sp": sp + shift_a(i)}, device_id_type=MESH)
        pl.semaphore_signal(barrier, inc=1, device_id={"sp": sp + shift_b(i)}, device_id_type=MESH)
    pl.semaphore_signal(barrier, inc=1, device_id={"sp": mate}, device_id_type=MESH)
    pl.semaphore_wait(barrier, 3 * (RING - 1) + 1)

    pending = []

    def send(src, dst, send_sem, recv_sem, where):
        return pltpu.make_async_remote_copy(
            src_ref=src,
            dst_ref=dst,
            send_sem=send_sem,
            recv_sem=recv_sem,
            device_id=where,
            device_id_type=MESH,
        )

    def go(copy):
        copy.start()
        pending.append(copy)

    def part(i):
        return slice(i * half, (i + 1) * half)

    def token_copy(block, i, slot, where, src=None):
        src = tok.at[block, part(i)] if src is None else src
        return send(src, tok.at[block, part(i)], tok_send.at[slot], tok_recv.at[block, i], {"tp": where})

    go(token_copy(tp, 0, 0, right, tok_hbm.at[part(0)]))
    go(token_copy(tp, 1, 1, left, tok_hbm.at[part(1)]))
    go(token_copy(tp, 1, 2, right, tok_hbm.at[part(1)]))
    go(token_copy(tp, 0, 3, left, tok_hbm.at[part(0)]))

    gains[...] = jnp.zeros_like(gains)
    gains[0:heads, 0:width] = qg_ref[...].astype(F32) * (LOG2E * width ** (-0.5))
    gains[heads : heads + 1, 0:width] = kg_ref[...].astype(F32)
    turned_gains = jnp.transpose(gains[...])
    top[...] = jnp.full_like(top, -1e30)
    acc[...] = jnp.zeros_like(acc)
    turned_v[:, width:, :] = jnp.ones_like(turned_v[:, width:, :])

    def project(block):
        piece = tok[block]
        at = pl.ds(pl.multiple_of(block * rows, rows), rows)
        raw[at, 0:query_cols] = jnp.dot(piece, wq[...], preferred_element_type=F32)
        raw[at, query_cols:] = lax.dot_general(
            piece, wkv[...], (((1,), (1,)), ((), ())), preferred_element_type=F32
        )

    sizes = (rows, 2 * rows, rows)
    bases = (0, n_sp * rows, 3 * n_sp * rows)

    def make_kv(block, p, offset):
        at = pl.ds(pl.multiple_of(block * rows, rows), rows)
        turned = jnp.transpose(raw[at, query_cols:])
        angles = angle_tables(sp * count + block * rows, rows, width // 4)
        keys = prepare(turned[0:width], turned_gains[0:width, heads : heads + 1], angles)
        to = pl.ds(pl.multiple_of(bases[p] + sp * sizes[p] + offset, rows), rows)
        kv[to, 0:width] = jnp.transpose(keys).astype(BF16)
        kv[to, width : 2 * width] = raw[at, query_cols + width :].astype(BF16)

    def kv_copy(block, p, slot, where):
        spot = kv.at[pl.ds(pl.multiple_of(bases[p] + block * sizes[p], rows), sizes[p])]
        return send(spot, spot, kv_send.at[p, slot], kv_recv.at[block, p], {"sp": where})

    def own_send(p):
        for i in range(1, RING):
            go(kv_copy(sp, p, i - 1, sp + shift_a(i)))
        for i in range(1, RING):
            go(kv_copy(sp, p, i + 2, sp + shift_b(i)))
        go(kv_copy(sp, p, 6, mate))

    def spread_copies(p):
        for k in range(1, RING):
            block = sp + shift_a(k)
            yield [
                kv_copy(block, p, 7 + (k - 1) * RING + j - 1, sp + shift_b(j)) for j in range(1, RING)
            ] + [kv_copy(block, p, 7 + (k - 1) * RING + RING - 1, mate)]

    def spread(p):
        for copies in spread_copies(p):
            copies[0].wait_recv()
            for copy in copies:
                copy.start()

    def hand_copies(p):
        for j in range(1, RING):
            for k in range(RING):
                yield kv_copy(sp + shift_a(k) + shift_b(j), p, 19 + (j - 1) * RING + k, mate)

    def hand(p):
        for copy in hand_copies(p):
            copy.wait_recv()
            copy.start()

    def from_mate(p):
        for chip in range(RING * RING):
            kv_copy(2 * chip + 1 - core, p, 0, mate).wait_recv()

    quarter = group // 4

    def wo_at(block, side, i):
        return wo.at[block, pl.ds(pl.multiple_of(side * 2 * quarter + i * quarter, quarter), quarter)]

    def wo_copy(block, side, i, slot, where):
        spot = wo_at(block, side, i)
        return send(spot, spot, wo_send.at[slot], wo_recv.at[block, side, i], where)

    def wo_first():
        return [
            wo_copy(tp, core, 0, 0, {"tp": right}),
            wo_copy(tp, core, 1, 1, {"tp": left}),
            wo_copy(tp, core, 1, 2, {"tp": right}),
            wo_copy(tp, core, 0, 3, {"tp": left}),
        ]

    def wo_forward():
        return [wo_copy(left, core, 0, 4, {"tp": right}), wo_copy(right, core, 1, 5, {"tp": left})]

    hand_order = ((left, 0), (right, 1), (left, 1), (right, 0), (opposite, 0), (opposite, 1))

    def wo_hand(n):
        block, i = hand_order[n]
        return wo_copy(block, core, i, 6 + n, {"sp": mate})

    loads[2].wait()
    loads[3].wait()
    loads[1].wait()
    loads[0].wait()
    project(tp)
    make_kv(tp, 0, 0)
    own_send(0)
    token_copy(left, 0, 0, right).wait_recv()
    go(token_copy(left, 0, 4, right))
    token_copy(right, 1, 0, left).wait_recv()
    go(token_copy(right, 1, 5, left))
    spread(0)
    token_copy(left, 1, 0, right).wait_recv()
    project(left)
    make_kv(left, 1, 0)
    token_copy(right, 0, 0, left).wait_recv()
    project(right)
    make_kv(right, 1, rows)
    own_send(1)
    hand(0)
    spread(1)
    loads[4].wait()
    token_copy(opposite, 0, 0, right).wait_recv()
    token_copy(opposite, 1, 0, left).wait_recv()
    for copy in wo_first():
        copy.start()
    project(opposite)
    make_kv(opposite, 2, 0)
    own_send(2)

    tables = angle_tables(sp * count, count, width // 4)
    turned = jnp.transpose(raw[:, 0:query_cols])
    for h in range(heads):
        q = prepare(turned[h * width : (h + 1) * width], turned_gains[0:width, h : h + 1], tables)
        queries[:, h * count : (h + 1) * count] = q.astype(BF16)
    from_mate(0)

    def turn(chunk, slot):
        at = pl.ds(pl.multiple_of(chunk * CHUNK, CHUNK), CHUNK)
        turned_v[slot, 0:width] = jnp.transpose(kv[at])[width : 2 * width]

    def score(chunk, t, slot, i):
        at = pl.ds(pl.multiple_of(chunk * CHUNK + i * SUB, SUB), SUB)
        s = jnp.dot(kv[at, 0:width], queries[:, t * TILE : (t + 1) * TILE], preferred_element_type=F32)
        scores[slot, i * SUB : (i + 1) * SUB] = s
        return jnp.max(s.reshape(SUB // 8, 8, TILE), axis=0)

    def score_all(chunk, t, slot):
        best = None
        for i in range(CHUNK // SUB):
            m = score(chunk, t, slot, i)
            best = m if best is None else jnp.maximum(best, m)
        peak[slot] = best

    turn(0, 0)
    score_all(0, 0, 0)
    score_all(0, 1, 1)

    def step(j, carry):
        @pl.when(j == 1)
        def _():
            spread(2)

        @pl.when(j == 2)
        def _():
            hand(1)

        @pl.when(j == 3)
        def _():
            from_mate(1)

        @pl.when(j == 6)
        def _():
            for copy, n in zip(wo_forward(), (0, 1)):
                copy.wait_recv()
                copy.start()
                wo_hand(n).start()
            hand(2)

        @pl.when(j == 11)
        def _():
            from_mate(2)

        @pl.when(j == 13)
        def _():
            for n in (2, 3):
                wo_hand(n).wait_recv()
                wo_hand(n).start()

        now = lax.rem(j, 2)
        later = lax.rem(j + 1, n_chunks)
        for t in range(n_tiles):
            if t == 1:
                turn(later, 1 - now)
            chunk, tile = (j, t + 2) if t + 2 < n_tiles else (later, t + 2 - n_tiles)
            fill, slot = (t + 2) % 3, t % 3
            old = top[t]
            new = jnp.maximum(old, jnp.max(peak[slot], axis=0, keepdims=True))
            best = None
            total = None
            for i in range(CHUNK // SUB):
                m = score(chunk, tile, fill, i)
                best = m if best is None else jnp.maximum(best, m)
                at = slice(i * SUB, (i + 1) * SUB)
                weights = jnp.exp2(scores[slot, at] - new).astype(BF16)
                mixed = jnp.dot(turned_v[now, :, at], weights, preferred_element_type=F32)
                total = mixed if total is None else total + mixed
            peak[fill] = best
            acc[t] = acc[t] * jnp.exp2(old - new) + total
            top[t] = new
        return carry

    lax.fori_loop(0, n_chunks, step, 0)

    for n in (4, 5):
        wo_hand(n).wait_recv()
        wo_hand(n).start()

    flat = [acc[t] for t in range(n_tiles)]
    sums = jnp.concatenate([f[width : width + 1] for f in flat], axis=1)
    outs = jnp.concatenate([f[0:width] / f[width : width + 1] for f in flat], axis=1)
    logs = (jnp.concatenate([top[t] for t in range(n_tiles)], axis=1) + jnp.log2(sums)) * LN2
    finished = []
    for h in range(heads):
        at = slice(h * count, (h + 1) * count)
        finished.append(outs[:, at])
        log_ref[h : h + 1, :] = logs[:, at]
    att[...] = jnp.transpose(jnp.concatenate(finished, axis=0)).astype(BF16)

    def att_copy(i):
        to = lax.rem(tp + i, RING)
        src = att.at[pl.ds(pl.multiple_of(to * rows, rows), rows)]
        return send(src, att_in.at[tp], att_send.at[i - 1], att_recv.at[tp], {"tp": to})

    for i in (2, 1, 3):
        att_copy(i).start()

    def att_wait(block):
        send(att_in.at[block], att_in.at[block], att_send.at[0], att_recv.at[block], {"tp": right}).wait_recv()

    for block, i in hand_order:
        wo_copy(block, 1 - core, i, 0, {"sp": mate}).wait_recv()
    own = att[pl.ds(pl.multiple_of(tp * rows, rows), rows)]
    for block in (left, right, opposite):
        att_wait(block)
    model = mixed_ref.shape[1]
    cols = 512
    for n in range(model // cols):
        at = slice(n * cols, (n + 1) * cols)
        total = jnp.dot(own, wo[tp, :, at], preferred_element_type=F32)
        for block in (left, right, opposite):
            total = total + jnp.dot(att_in[block], wo[block, :, at], preferred_element_type=F32)
        mixed_ref[:, at] = total.astype(BF16)

    for copy in pending:
        copy.wait_send()
    for p in (0, 1, 2):
        for copies in spread_copies(p):
            for copy in copies:
                copy.wait_send()
        for copy in hand_copies(p):
            copy.wait_send()
    for copy in wo_first() + wo_forward() + [wo_hand(n) for n in range(6)]:
        copy.wait_send()
    for i in range(1, RING):
        att_copy(i).wait_send()


def body(tokens, query_weight, key_weight, value_weight, out_weight, query_gain, key_gain):
    rows, depth = tokens.shape
    query_cols = query_weight.shape[1]
    kv_cols = key_weight.shape[1]
    heads, width = query_gain.shape
    group, model = out_weight.shape
    count = rows * RING
    n_sp = RING * RING * 2
    n_tiles = heads * count // TILE
    any_space = pl.BlockSpec(memory_space=pl.ANY)
    vmem = pl.BlockSpec(memory_space=pltpu.VMEM)
    dma = pltpu.SemaphoreType.DMA
    return pl.pallas_call(
        kernel,
        out_shape=(
            pltpu.VMEM((rows, model), BF16),
            pltpu.VMEM((heads, count), F32),
        ),
        in_specs=[any_space] * 5 + [vmem] * 2,
        out_specs=(vmem, vmem),
        scratch_shapes=[
            pltpu.VMEM((RING, rows, depth), BF16),
            pltpu.VMEM((depth, query_cols), BF16),
            pltpu.VMEM((2 * kv_cols, depth), BF16),
            pltpu.VMEM((RING, group, model), BF16),
            pltpu.VMEM((128, 128), F32),
            pltpu.VMEM((count, query_cols + 2 * kv_cols), F32),
            pltpu.VMEM((width, heads * count), BF16),
            pltpu.VMEM((n_sp * count, 2 * width), BF16),
            pltpu.VMEM((3, CHUNK, TILE), F32),
            pltpu.VMEM((3, 8, TILE), F32),
            pltpu.VMEM((2, width + ONES, CHUNK), BF16),
            pltpu.VMEM((n_tiles, width + ONES, TILE), F32),
            pltpu.VMEM((n_tiles, 1, TILE), F32),
            pltpu.VMEM((count, group), BF16),
            pltpu.VMEM((RING, rows, group), BF16),
            dma((5,)),
            dma((6,)),
            dma((RING, 2)),
            dma((3, 31)),
            dma((n_sp, 3)),
            dma((12,)),
            dma((RING, 2, 2)),
            dma((RING - 1,)),
            dma((RING,)),
        ],
        compiler_params=pltpu.CompilerParams(
            collective_id=0, has_side_effects=True, vmem_limit_bytes=60 * 1024 * 1024
        ),
        name="attention",
    )(tokens, query_weight, key_weight.T, value_weight.T, out_weight, query_gain, key_gain)


def solution(mesh):
    return jax.shard_map(
        body,
        mesh=mesh,
        in_specs=(
            P(("sp", "tp"), None),
            P(None, "tp"),
            P(None, "tp"),
            P(None, "tp"),
            P("tp", None),
            P("tp", None),
            P("tp", None),
        ),
        out_specs=(P(("sp", "tp"), None), P("tp", "sp")),
        check_vma=False,
    )
```

```python
import functools
import math

import jax
import jax.numpy as jnp
from jax import lax
from jax.experimental import pallas as pl
from jax.experimental.pallas import tpu as pltpu
from jax.sharding import PartitionSpec as P

GRID_W = 64
ROPE_BASE = 10000.0
EPS = 1e-06
LOG2E = math.log2(math.e)
LN2 = math.log(2.0)
ONES = 16
RING = 4
CHUNK = 768
TILE = 256
SUB = 256
MESH = pl.DeviceIdType.MESH
F32 = jnp.float32
BF16 = jnp.bfloat16


def prepare(x, gain, tables):
    quarter = x.shape[0] // 4
    x = x * lax.rsqrt(jnp.mean(x * x, axis=0, keepdims=True) + EPS) * gain
    a, b, c, d = (x[i * quarter : (i + 1) * quarter] for i in range(4))
    row_cos, row_sin, col_cos, col_sin = tables
    return jnp.concatenate(
        [
            a * row_cos - b * row_sin,
            b * row_cos + a * row_sin,
            c * col_cos - d * col_sin,
            d * col_cos + c * col_sin,
        ],
        axis=0,
    )


def kernel(
    tok_hbm,
    wq_hbm,
    wk_hbm,
    wv_hbm,
    wo_hbm,
    qg_ref,
    kg_ref,
    mixed_ref,
    log_ref,
    tok,
    wq,
    wkv,
    wo,
    gain_cols,
    tables,
    queries,
    kv,
    scores,
    peak,
    turned_v,
    acc,
    top,
    att,
    att_in,
    log_rows,
    product,
    local_sem,
    tok_send,
    tok_recv,
    kv_send,
    kv_recv,
    wo_send,
    wo_recv,
    att_send,
    att_recv,
):
    sp = lax.axis_index("sp")
    tp = lax.axis_index("tp")
    core = lax.rem(sp, 2)
    y = lax.rem(sp // 2, RING)
    z = sp // (2 * RING)
    mate = sp + 1 - 2 * core
    left, right, opposite = (lax.rem(tp + i, RING) for i in (3, 1, 2))
    rows = tok.shape[1]
    half = rows // 2
    heads, width = qg_ref.shape
    count = rows * RING
    kv_cols = wk_hbm.shape[0]
    group, model = wo_hbm.shape
    n_tiles = 2 * heads * rows // TILE

    coord_a = y * (1 - core) + z * core
    step_a = 2 + 6 * core
    coord_b = z * (1 - core) + y * core
    step_b = 8 - 6 * core

    def peer_a(i):
        return {"sp": sp + (lax.rem(coord_a + i, RING) - coord_a) * step_a}

    def peer_b(i):
        return {"sp": sp + (lax.rem(coord_b + i, RING) - coord_b) * step_b}

    loads = [
        pltpu.make_async_copy(src, dst, local_sem.at[i])
        for i, (src, dst) in enumerate(
            (
                (tok_hbm, tok.at[0]),
                (wk_hbm, wkv.at[0:kv_cols]),
                (wv_hbm, wkv.at[kv_cols:]),
                (wq_hbm, wq),
                (wo_hbm, wo.at[0]),
            )
        )
    ]
    for load in loads:
        load.start()

    barrier = pltpu.get_barrier_semaphore()
    for i in range(1, RING):
        pl.semaphore_signal(barrier, inc=1, device_id={"tp": lax.rem(tp + i, RING)}, device_id_type=MESH)
        pl.semaphore_signal(barrier, inc=1, device_id=peer_a(i), device_id_type=MESH)
        pl.semaphore_signal(barrier, inc=1, device_id=peer_b(i), device_id_type=MESH)
    pl.semaphore_signal(barrier, inc=1, device_id={"sp": mate}, device_id_type=MESH)
    pl.semaphore_wait(barrier, 3 * (RING - 1) + 1)

    def send(src, dst, send_sem, recv_sem, where):
        return pltpu.make_async_remote_copy(
            src_ref=src,
            dst_ref=dst,
            send_sem=send_sem,
            recv_sem=recv_sem,
            device_id=where,
            device_id_type=MESH,
        )

    def part(i):
        return slice(i * half, (i + 1) * half)

    to_left, to_right, to_opposite, to_mate = {"tp": left}, {"tp": right}, {"tp": opposite}, {"sp": mate}

    def token_copy(src, piece, i, slot, where):
        return send(src, tok.at[piece, part(i)], tok_send.at[slot], tok_recv.at[piece, i], where)

    first_half, second_half = tok_hbm.at[part(0)], tok_hbm.at[part(1)]
    token_out = [
        token_copy(first_half, 1, 0, 0, to_right),
        token_copy(second_half, 1, 1, 1, to_left),
        token_copy(second_half, 2, 0, 2, to_right),
        token_copy(first_half, 2, 1, 3, to_left),
    ]
    token_on = [
        token_copy(tok.at[1, part(0)], 3, 0, 4, to_right),
        token_copy(tok.at[1, part(1)], 3, 1, 5, to_left),
    ]
    for copy in token_out:
        copy.start()

    def token_wait(piece, i):
        token_copy(tok.at[1, part(i)], piece, i, 4 + i, to_right).wait_recv()

    starts = (
        (tp * rows, tp * rows + half),
        (left * rows, right * rows + half),
        (left * rows + half, right * rows),
        (opposite * rows, opposite * rows + half),
    )

    quarter = width // 4
    lane = lax.broadcasted_iota(jnp.int32, (quarter, heads * rows), 1)
    spot = lane
    for h in range(1, heads):
        spot = spot - jnp.where(lane >= h * rows, rows, 0)
    order = lax.broadcasted_iota(jnp.int32, (quarter, heads * rows), 0).astype(F32)
    freq = jnp.exp(order * (-math.log(ROPE_BASE) / quarter))
    shift = GRID_W.bit_length() - 1
    for p in range(4):
        a, b = starts[p]
        place = sp * count + spot + jnp.where(spot < half, a, b - half)
        row = lax.shift_right_logical(place, shift).astype(F32) * freq
        col = jnp.bitwise_and(place, GRID_W - 1).astype(F32) * freq
        tables[p, 0:quarter] = jnp.cos(row)
        tables[p, quarter : 2 * quarter] = jnp.sin(row)
        tables[p, 2 * quarter : 3 * quarter] = jnp.cos(col)
        tables[p, 3 * quarter :] = jnp.sin(col)

    gain_rows = [
        jnp.broadcast_to(qg_ref[h : h + 1, :].astype(F32) * (LOG2E * width ** (-0.5)), (rows, width))
        for h in range(heads)
    ]
    gain_rows.append(jnp.broadcast_to(kg_ref[...].astype(F32), (128, width)))
    gain_cols[...] = jnp.transpose(jnp.concatenate(gain_rows, axis=0))
    top[...] = jnp.full_like(top, -1e30)
    acc[...] = jnp.zeros_like(acc)
    turned_v[:, width:, :] = jnp.ones_like(turned_v[:, width:, :])
    log_rows[...] = jnp.zeros_like(log_rows)

    def kv_rows(p, j, c, k):
        return pl.ds(pl.multiple_of((((p * RING + j) * 2 + c) * RING + k) * rows, rows), rows)

    def tables_of(p, n):
        return [tables[p, i * quarter : (i + 1) * quarter, 0:n] for i in range(4)]

    def make_kv(p):
        raw = lax.dot_general(tok[p], wkv[...], (((1,), (1,)), ((), ())), preferred_element_type=F32)
        turned = jnp.transpose(raw)
        gain = gain_cols[:, heads * rows : heads * rows + rows]
        keys = prepare(turned[0:width], gain, tables_of(p, rows))
        to = kv_rows(p, 0, core, 0)
        kv[to, 0:width] = jnp.transpose(keys).astype(BF16)
        kv[to, width : 2 * width] = raw[:, width:].astype(BF16)

    def make_queries(p):
        raw = jnp.dot(tok[p], wq[...], preferred_element_type=F32)
        stacked = jnp.concatenate([raw[:, h * width : (h + 1) * width] for h in range(heads)], axis=0)
        q = prepare(jnp.transpose(stacked), gain_cols[:, 0 : heads * rows], tables_of(p, heads * rows))
        at = slice((p % 2) * heads * rows, (p % 2 + 1) * heads * rows)
        queries[p // 2, :, at] = q.astype(BF16)

    def kv_copy(p, j, k, to_j, to_k, slot, where):
        return send(
            kv.at[kv_rows(p, j, core, k)],
            kv.at[kv_rows(p, to_j, core, to_k)],
            kv_send.at[p, slot],
            kv_recv.at[p, to_j, core, to_k],
            where,
        )

    def own_copies(p):
        copies = [kv_copy(p, 0, 0, 0, RING - i, i - 1, peer_a(i)) for i in range(1, RING)]
        copies += [kv_copy(p, 0, 0, RING - i, 0, i + 2, peer_b(i)) for i in range(1, RING)]
        return copies + [kv_copy(p, 0, 0, 0, 0, 6, to_mate)]

    def spread_copies(p, k):
        base = 7 + (k - 1) * RING
        copies = [kv_copy(p, 0, k, RING - i, k, base + i - 1, peer_b(i)) for i in range(1, RING)]
        return copies + [kv_copy(p, 0, k, 0, k, base + RING - 1, to_mate)]

    def hand_copies(p, j):
        return [kv_copy(p, j, k, j, k, 19 + (j - 1) * RING + k, to_mate) for k in range(RING)]

    def own_send(p):
        for copy in own_copies(p):
            copy.start()

    def spread(p):
        for k in (1, 3, 2):
            copies = spread_copies(p, k)
            copies[-1].wait_recv()
            for copy in copies:
                copy.start()

    def hand(p, j):
        for copy in hand_copies(p, j):
            copy.wait_recv()
            copy.start()

    def from_mate(p, j):
        for k in range(RING):
            spot = kv.at[kv_rows(p, j, 1 - core, k)]
            send(spot, spot, kv_send.at[p, 0], kv_recv.at[p, j, 1 - core, k], to_mate).wait_recv()

    piece_rows = group // 4

    def wo_copy(block, to_block, side, i, slot, where):
        at = pl.ds(pl.multiple_of((side * 2 + i) * piece_rows, piece_rows), piece_rows)
        return send(
            wo.at[block, at], wo.at[to_block, at], wo_send.at[slot], wo_recv.at[to_block, side, i], where
        )

    wo_out = [
        wo_copy(0, 1, core, 0, 0, to_right),
        wo_copy(0, 2, core, 1, 1, to_left),
        wo_copy(0, 1, core, 1, 2, to_right),
        wo_copy(0, 2, core, 0, 3, to_left),
    ]
    wo_on = [wo_copy(1, 3, core, 0, 4, to_right), wo_copy(2, 3, core, 1, 5, to_left)]
    wo_order = ((1, 0), (2, 1), (1, 1), (2, 0), (3, 0), (3, 1))
    wo_hand = [wo_copy(block, block, core, i, 6 + n, to_mate) for n, (block, i) in enumerate(wo_order)]

    def piece_work(p):
        make_kv(p)
        own_send(p)
        make_queries(p)

    loads[0].wait()
    loads[1].wait()
    loads[2].wait()
    make_kv(0)
    own_send(0)
    loads[3].wait()
    make_queries(0)
    spread(0)
    for i, copy in enumerate(token_on):
        token_wait(1, i)
        copy.start()
    piece_work(1)
    from_mate(0, 0)

    def turn(chunk, slot):
        at = pl.ds(pl.multiple_of(chunk * CHUNK, CHUNK), CHUNK)
        turned_v[slot, 0:width] = jnp.transpose(kv[at])[width : 2 * width]

    def score(chunk, side, t, slot, i):
        at = pl.ds(pl.multiple_of(chunk * CHUNK + i * SUB, SUB), SUB)
        q = queries[side, :, t * TILE : (t + 1) * TILE]
        s = jnp.dot(kv[at, 0:width], q, preferred_element_type=F32)
        scores[slot, i * SUB : (i + 1) * SUB] = s
        return jnp.max(s.reshape(SUB // 8, 8, TILE), axis=0)

    def score_all(chunk, side, t, slot):
        best = None
        for i in range(CHUNK // SUB):
            m = score(chunk, side, t, slot, i)
            best = m if best is None else jnp.maximum(best, m)
        peak[slot] = best

    n_steps = 2 * 4 * RING

    def chunk_of(s):
        late = s // 16
        return (1 - late) * lax.rem(s, 8) + late * (8 + 4 * (lax.rem(s, 16) // 8) + lax.rem(s, 4))

    def side_of(s):
        late = s // 16
        return (1 - late) * (s // 8) + late * (1 - lax.rem(s // 4, 2))

    turn(0, 0)
    score_all(0, 0, 0, 0)
    score_all(0, 0, 1, 1)

    def finish(side):
        flat = [acc[side, t] for t in range(n_tiles)]
        sums = jnp.concatenate([f[width : width + 8] for f in flat], axis=1)
        tops = jnp.concatenate([top[side, t] for t in range(n_tiles)], axis=1)
        outs = jnp.concatenate([f[0:width] / f[width : width + 1] for f in flat], axis=1)
        logs = (tops + jnp.log2(sums)) * LN2
        turned = jnp.transpose(jnp.concatenate([outs, logs], axis=0))
        for q in range(2):
            p = 2 * side + q
            for h in range(heads):
                base = (q * heads + h) * rows
                att[p, :, h * width : (h + 1) * width] = turned[base : base + rows, 0:width].astype(BF16)
        return turned

    def keep_logs(side, turned):
        for q in range(2):
            for h in range(heads):
                for i in range(2):
                    base = (q * heads + h) * rows + i * half
                    to = pl.ds(pl.multiple_of(starts[2 * side + q][i], half), half)
                    log_rows[to, h : h + 1] = turned[base : base + half, width : width + 1]

    def att_copy(p, i, source, at, slot, where):
        src = att.at[p] if i is None else att.at[p, part(i)]
        dst = att_in.at[source] if at is None else att_in.at[source, part(at)]
        return send(src, dst, att_send.at[slot], att_recv.at[source, at or 0], where)

    att_late = [
        att_copy(3, None, 2, None, 0, to_opposite),
        att_copy(2, 0, 1, 1, 1, to_left),
        att_copy(2, 1, 0, 0, 2, to_right),
    ]
    att_last = [att_copy(1, 0, 1, 0, 3, to_left), att_copy(1, 1, 0, 1, 4, to_right)]

    def at_step(s, now, acts):
        @pl.when(s == now)
        def _():
            for act in acts:
                act()

    def wait_tokens(p):
        for i in range(2):
            token_wait(p, i)

    def start_wo():
        loads[4].wait()
        for copy in wo_out:
            copy.start()

    def wo_first():
        for n in range(2):
            wo_hand[n].wait_recv()
            wo_on[n].start()
            wo_hand[n].start()

    def close_late():
        keep_logs(1, finish(1))
        for copy in att_late:
            copy.start()

    def later(f, *args):
        return functools.partial(f, *args)

    duties = {
        0: [later(hand, 0, j) for j in (1, 2, 3)] + [later(from_mate, 0, 1)],
        1: [later(wait_tokens, 2), later(piece_work, 2), later(spread, 1), later(from_mate, 0, 2)],
        2: [later(from_mate, 0, 3)],
        3: [later(from_mate, 1, 0)],
        4: [later(hand, 1, j) for j in (1, 2, 3)] + [later(from_mate, 1, 1)],
        5: [later(from_mate, 1, 2), later(spread, 2)],
        6: [later(from_mate, 1, 3)],
        7: [later(wait_tokens, 3), later(piece_work, 3), start_wo],
        12: [later(hand, 2, j) for j in (1, 2, 3)],
        13: [later(spread, 3)],
        15: [later(from_mate, 2, 0)],
        16: [later(from_mate, 2, 1)],
        17: [later(from_mate, 2, 2)],
        18: [later(from_mate, 2, 3)],
        21: [later(hand, 3, j) for j in (1, 2, 3)],
        22: [wo_first],
        23: [later(from_mate, 3, 0)],
        24: [later(from_mate, 3, 1)],
        25: [later(from_mate, 3, 2)],
        26: [later(from_mate, 3, 3)],
        28: [close_late],
    }

    def step(s, carry):
        for now, acts in duties.items():
            if acts:
                at_step(s, now, acts)
        slot_v = lax.rem(s, 2)
        after = lax.rem(s + 1, n_steps)
        chunk, side = chunk_of(s), side_of(s)
        next_chunk, next_side = chunk_of(after), side_of(after)
        for t in range(n_tiles):
            if t == 1:
                turn(next_chunk, 1 - slot_v)
            ahead = t + 2
            to_chunk, to_side = (chunk, side) if ahead < n_tiles else (next_chunk, next_side)
            tile, fill, slot = ahead % n_tiles, ahead % 3, t % 3
            old = top[side, t]
            new = jnp.maximum(old, jnp.max(peak[slot], axis=0, keepdims=True))
            best = None
            total = None
            for i in range(CHUNK // SUB):
                m = score(to_chunk, to_side, tile, fill, i)
                best = m if best is None else jnp.maximum(best, m)
                at = slice(i * SUB, (i + 1) * SUB)
                weights = jnp.exp2(scores[slot, at] - new).astype(BF16)
                mixed = jnp.dot(turned_v[slot_v, :, at], weights, preferred_element_type=F32)
                total = mixed if total is None else total + mixed
            peak[fill] = best
            acc[side, t] = acc[side, t] * jnp.exp2(old - new) + total
            top[side, t] = new
        return carry

    lax.fori_loop(0, n_steps, step, 0)

    turned = finish(0)
    for copy in att_last:
        copy.start()
    keep_logs(0, turned)
    log_ref[...] = jnp.transpose(log_rows[...])[0:heads]

    for n in range(2, 6):
        wo_hand[n].wait_recv()
        wo_hand[n].start()
    for block, i in wo_order:
        wo_copy(block, block, 1 - core, i, 0, to_mate).wait_recv()

    cols = 512

    def columns(n):
        return slice(n * cols, (n + 1) * cols)

    def times(x, block, n):
        return jnp.dot(x, wo[block, :, columns(n)], preferred_element_type=F32)

    att_late[0].wait_recv()
    for n in range(model // cols):
        product[:, columns(n)] = times(att[0], 0, n) + times(att_in[2], 3, n)
    for copy in att_late[1:] + att_last:
        copy.wait_recv()
    for n in range(model // cols):
        total = product[:, columns(n)] + times(att_in[0], 1, n) + times(att_in[1], 2, n)
        mixed_ref[:, columns(n)] = total.astype(BF16)

    for copy in token_out + token_on + wo_out + wo_on + wo_hand + att_late + att_last:
        copy.wait_send()
    for p in range(4):
        copies = own_copies(p)
        for k in range(1, RING):
            copies += spread_copies(p, k) + hand_copies(p, k)
        for copy in copies:
            copy.wait_send()


def body(tokens, query_weight, key_weight, value_weight, out_weight, query_gain, key_gain):
    rows, depth = tokens.shape
    query_cols = query_weight.shape[1]
    kv_cols = key_weight.shape[1]
    heads, width = query_gain.shape
    group, model = out_weight.shape
    count = rows * RING
    n_sp = RING * RING * 2
    n_tiles = 2 * heads * rows // TILE
    any_space = pl.BlockSpec(memory_space=pl.ANY)
    vmem = pl.BlockSpec(memory_space=pltpu.VMEM)
    dma = pltpu.SemaphoreType.DMA
    return pl.pallas_call(
        kernel,
        out_shape=(
            pltpu.VMEM((rows, model), BF16),
            pltpu.VMEM((heads, count), F32),
        ),
        in_specs=[any_space] * 5 + [vmem] * 2,
        out_specs=(vmem, vmem),
        scratch_shapes=[
            pltpu.VMEM((4, rows, depth), BF16),
            pltpu.VMEM((depth, query_cols), BF16),
            pltpu.VMEM((2 * kv_cols, depth), BF16),
            pltpu.VMEM((4, group, model), BF16),
            pltpu.VMEM((width, heads * rows + 128), F32),
            pltpu.VMEM((4, width, heads * rows), F32),
            pltpu.VMEM((2, width, 2 * heads * rows), BF16),
            pltpu.VMEM((n_sp * count, 2 * width), BF16),
            pltpu.VMEM((3, CHUNK, TILE), F32),
            pltpu.VMEM((3, 8, TILE), F32),
            pltpu.VMEM((2, width + ONES, CHUNK), BF16),
            pltpu.VMEM((2, n_tiles, width + ONES, TILE), F32),
            pltpu.VMEM((2, n_tiles, 1, TILE), F32),
            pltpu.VMEM((4, rows, group), BF16),
            pltpu.VMEM((3, rows, group), BF16),
            pltpu.VMEM((count, 128), F32),
            pltpu.VMEM((rows, model), F32),
            dma((5,)),
            dma((6,)),
            dma((4, 2)),
            dma((4, 31)),
            dma((4, RING, 2, RING)),
            dma((12,)),
            dma((4, 2, 2)),
            dma((5,)),
            dma((3, 2)),
        ],
        compiler_params=pltpu.CompilerParams(
            collective_id=0, has_side_effects=True, vmem_limit_bytes=60 * 1024 * 1024
        ),
        name="attention",
    )(tokens, query_weight, key_weight.T, value_weight.T, out_weight, query_gain, key_gain)


def solution(mesh):
    return jax.shard_map(
        body,
        mesh=mesh,
        in_specs=(
            P(("sp", "tp"), None),
            P(None, "tp"),
            P(None, "tp"),
            P(None, "tp"),
            P("tp", None),
            P("tp", None),
            P("tp", None),
        ),
        out_specs=(P(("sp", "tp"), None), P("tp", "sp")),
        check_vma=False,
    )
```

```python
import functools
import math

import jax
import jax.numpy as jnp
from jax import lax
from jax.experimental import pallas as pl
from jax.experimental.pallas import tpu as pltpu
from jax.sharding import PartitionSpec as P

GRID_W = 64
ROPE_BASE = 10000.0
EPS = 1e-06
LOG2E = math.log2(math.e)
LN2 = math.log(2.0)
ONES = 16
RING = 4
CHUNK = 768
TILE = 256
SUB = 256
MESH = pl.DeviceIdType.MESH
F32 = jnp.float32
BF16 = jnp.bfloat16


def prepare(x, gain, tables):
    quarter = x.shape[0] // 4
    x = x * lax.rsqrt(jnp.mean(x * x, axis=0, keepdims=True) + EPS) * gain
    a, b, c, d = (x[i * quarter : (i + 1) * quarter] for i in range(4))
    row_cos, row_sin, col_cos, col_sin = tables
    return jnp.concatenate(
        [
            a * row_cos - b * row_sin,
            b * row_cos + a * row_sin,
            c * col_cos - d * col_sin,
            d * col_cos + c * col_sin,
        ],
        axis=0,
    )


def kernel(
    tok_hbm,
    wq_hbm,
    wk_hbm,
    wv_hbm,
    wo_hbm,
    qg_ref,
    kg_ref,
    mixed_ref,
    log_ref,
    tok,
    wq,
    wkv,
    wo,
    gain_cols,
    tables,
    queries,
    kv,
    scores,
    peak,
    turned_v,
    acc,
    top,
    att,
    att_in,
    log_rows,
    product,
    local_sem,
    tok_send,
    tok_recv,
    kv_send,
    kv_recv,
    wo_send,
    wo_recv,
    att_send,
    att_recv,
):
    sp = lax.axis_index("sp")
    tp = lax.axis_index("tp")
    core = lax.rem(sp, 2)
    y = lax.rem(sp // 2, RING)
    z = sp // (2 * RING)
    mate = sp + 1 - 2 * core
    left, right, opposite = (lax.rem(tp + i, RING) for i in (3, 1, 2))
    rows = tok.shape[1]
    half = rows // 2
    heads, width = qg_ref.shape
    count = rows * RING
    kv_cols = wk_hbm.shape[0]
    group, model = wo_hbm.shape
    n_tiles = 2 * heads * rows // TILE

    coord_a = y * (1 - core) + z * core
    step_a = 2 + 6 * core
    coord_b = z * (1 - core) + y * core
    step_b = 8 - 6 * core

    def peer_a(i):
        return {"sp": sp + (lax.rem(coord_a + i, RING) - coord_a) * step_a}

    def peer_b(i):
        return {"sp": sp + (lax.rem(coord_b + i, RING) - coord_b) * step_b}

    loads = [
        pltpu.make_async_copy(src, dst, local_sem.at[i])
        for i, (src, dst) in enumerate(
            (
                (tok_hbm, tok.at[0]),
                (wk_hbm, wkv.at[0:kv_cols]),
                (wv_hbm, wkv.at[kv_cols:]),
                (wq_hbm, wq),
                (wo_hbm, wo.at[0]),
            )
        )
    ]
    for load in loads:
        load.start()

    barrier = pltpu.get_barrier_semaphore()
    for i in range(1, RING):
        pl.semaphore_signal(barrier, inc=1, device_id={"tp": lax.rem(tp + i, RING)}, device_id_type=MESH)
        pl.semaphore_signal(barrier, inc=1, device_id=peer_a(i), device_id_type=MESH)
        pl.semaphore_signal(barrier, inc=1, device_id=peer_b(i), device_id_type=MESH)
    pl.semaphore_signal(barrier, inc=1, device_id={"sp": mate}, device_id_type=MESH)
    pl.semaphore_wait(barrier, 3 * (RING - 1) + 1)

    def send(src, dst, send_sem, recv_sem, where):
        return pltpu.make_async_remote_copy(
            src_ref=src,
            dst_ref=dst,
            send_sem=send_sem,
            recv_sem=recv_sem,
            device_id=where,
            device_id_type=MESH,
        )

    def part(i):
        return slice(i * half, (i + 1) * half)

    to_left, to_right, to_opposite, to_mate = {"tp": left}, {"tp": right}, {"tp": opposite}, {"sp": mate}

    def token_copy(src, piece, i, slot, where):
        return send(src, tok.at[piece, part(i)], tok_send.at[slot], tok_recv.at[piece, i], where)

    first_half, second_half = tok_hbm.at[part(0)], tok_hbm.at[part(1)]
    token_out = [
        token_copy(first_half, 1, 0, 0, to_right),
        token_copy(second_half, 1, 1, 1, to_left),
        token_copy(second_half, 2, 0, 2, to_right),
        token_copy(first_half, 2, 1, 3, to_left),
    ]
    token_on = [
        token_copy(tok.at[1, part(0)], 3, 0, 4, to_right),
        token_copy(tok.at[1, part(1)], 3, 1, 5, to_left),
    ]
    for copy in token_out:
        copy.start()

    def token_wait(piece, i):
        token_copy(tok.at[1, part(i)], piece, i, 4 + i, to_right).wait_recv()

    starts = (
        (tp * rows, tp * rows + half),
        (left * rows, right * rows + half),
        (left * rows + half, right * rows),
        (opposite * rows, opposite * rows + half),
    )

    quarter = width // 4
    lane = lax.broadcasted_iota(jnp.int32, (quarter, heads * rows), 1)
    spot = lane
    for h in range(1, heads):
        spot = spot - jnp.where(lane >= h * rows, rows, 0)
    order = lax.broadcasted_iota(jnp.int32, (quarter, heads * rows), 0).astype(F32)
    freq = jnp.exp(order * (-math.log(ROPE_BASE) / quarter))
    shift = GRID_W.bit_length() - 1
    for p in range(4):
        a, b = starts[p]
        place = sp * count + spot + jnp.where(spot < half, a, b - half)
        row = lax.shift_right_logical(place, shift).astype(F32) * freq
        col = jnp.bitwise_and(place, GRID_W - 1).astype(F32) * freq
        tables[p, 0:quarter] = jnp.cos(row)
        tables[p, quarter : 2 * quarter] = jnp.sin(row)
        tables[p, 2 * quarter : 3 * quarter] = jnp.cos(col)
        tables[p, 3 * quarter :] = jnp.sin(col)

    gain_rows = [
        jnp.broadcast_to(qg_ref[h : h + 1, :].astype(F32) * (LOG2E * width ** (-0.5)), (rows, width))
        for h in range(heads)
    ]
    gain_rows.append(jnp.broadcast_to(kg_ref[...].astype(F32), (128, width)))
    gain_cols[...] = jnp.transpose(jnp.concatenate(gain_rows, axis=0))
    top[...] = jnp.full_like(top, -1e30)
    acc[...] = jnp.zeros_like(acc)
    turned_v[:, width:, :] = jnp.ones_like(turned_v[:, width:, :])
    log_rows[...] = jnp.zeros_like(log_rows)

    place_of = (0, 1, 3, 2)

    def kv_rows(p, shift, c, k, n):
        base = (((p * RING + place_of[shift]) * 2 + c) * RING + k) * rows
        return kv.at[pl.ds(pl.multiple_of(base, half), n)]

    def tables_of(p, n):
        return [tables[p, i * quarter : (i + 1) * quarter, 0:n] for i in range(4)]

    def make_kv(p):
        raw = lax.dot_general(tok[p], wkv[...], (((1,), (1,)), ((), ())), preferred_element_type=F32)
        turned = jnp.transpose(raw)
        gain = gain_cols[:, heads * rows : heads * rows + rows]
        keys = prepare(turned[0:width], gain, tables_of(p, rows))
        to = kv_rows(p, 0, core, 0, rows)
        to[:, 0:width] = jnp.transpose(keys).astype(BF16)
        to[:, width : 2 * width] = raw[:, width:].astype(BF16)

    def make_queries(p):
        raw = jnp.dot(tok[p], wq[...], preferred_element_type=F32)
        stacked = jnp.concatenate([raw[:, h * width : (h + 1) * width] for h in range(heads)], axis=0)
        q = prepare(jnp.transpose(stacked), gain_cols[:, 0 : heads * rows], tables_of(p, heads * rows))
        at = slice((p % 2) * heads * rows, (p % 2 + 1) * heads * rows)
        queries[p // 2, :, at] = q.astype(BF16)

    def kv_copy(src, dst, p, shift, c, where):
        return send(src, dst, kv_send.at[p], kv_recv.at[p, place_of[shift], c], where)

    whole = RING * rows

    def own_send(p):
        src = kv_rows(p, 0, core, 0, rows)
        for i in (1, 3, 2):
            kv_copy(src, kv_rows(p, 0, core, RING - i, rows), p, 0, core, peer_a(i)).start()

    def hand_copy(p, shift):
        spot = kv_rows(p, shift, core, 0, whole)
        return kv_copy(spot, spot, p, shift, core, to_mate)

    def spread(p):
        spot = kv_rows(p, 0, core, 1, whole - rows)
        kv_copy(spot, spot, p, 0, core, to_mate).wait_recv()
        src = kv_rows(p, 0, core, 0, whole)
        for i in (1, 3):
            kv_copy(src, kv_rows(p, RING - i, core, 0, whole), p, RING - i, core, peer_b(i)).start()
        hand_copy(p, 0).start()

    def relay(p):
        for shift, k, to in ((3, 0, 1), (1, 2, 3)):
            hand_copy(p, shift).wait_recv()
            src = kv_rows(p, shift, core, k, 2 * rows)
            kv_copy(src, kv_rows(p, 2, core, k, 2 * rows), p, 2, core, peer_b(to)).start()
            hand_copy(p, shift).start()

    def hand(p):
        hand_copy(p, 2).wait_recv()
        hand_copy(p, 2).start()

    def from_mate(p, shift):
        spot = kv_rows(p, shift, 1 - core, 0, whole)
        kv_copy(spot, spot, p, shift, 1 - core, to_mate).wait_recv()

    strip = group // 8
    parity = lax.rem(coord_a, 2)
    to_pair = {"sp": sp + (1 - 2 * parity) * step_a}

    def wo_rows(block, side, first, n):
        return wo.at[block, pl.ds(pl.multiple_of((side * 4 + first) * strip, strip), n * strip)]

    def wo_copy(block, to_block, i, slot, where):
        at = 2 * parity + i
        return send(
            wo_rows(block, core, at, 1), wo_rows(to_block, core, at, 1), wo_send.at[slot], wo_recv.at[to_block, i], where
        )

    wo_out = [
        wo_copy(0, 1, 0, 0, to_right),
        wo_copy(0, 2, 1, 1, to_left),
        wo_copy(0, 1, 1, 2, to_right),
        wo_copy(0, 2, 0, 3, to_left),
    ]
    wo_on = [wo_copy(1, 3, 0, 4, to_right), wo_copy(2, 3, 1, 5, to_left)]
    wo_rest = [wo_copy(0, 1, 1, 2, to_right), wo_copy(0, 2, 0, 3, to_left)]

    def pair_copy(block):
        spot = wo_rows(block, core, 2 * parity, 2)
        return send(spot, spot, wo_send.at[5 + block], wo_recv.at[block, 2], to_pair)

    def wo_hand(block):
        spot = wo_rows(block, core, 0, 4)
        return send(spot, spot, wo_send.at[8 + block], wo_recv.at[block, 3], to_mate)

    def piece_work(p):
        make_kv(p)
        own_send(p)
        make_queries(p)

    loads[0].wait()
    loads[1].wait()
    loads[2].wait()
    make_kv(0)
    own_send(0)
    loads[3].wait()
    make_queries(0)
    spread(0)
    for i, copy in enumerate(token_on):
        token_wait(1, i)
        copy.start()
    loads[4].wait()
    for copy in wo_out:
        copy.start()
    piece_work(1)
    relay(0)
    from_mate(0, 0)

    def turn(chunk, slot):
        at = pl.ds(pl.multiple_of(chunk * CHUNK, CHUNK), CHUNK)
        turned_v[slot, 0:width] = jnp.transpose(kv[at])[width : 2 * width]

    def score(chunk, side, t, slot, i):
        at = pl.ds(pl.multiple_of(chunk * CHUNK + i * SUB, SUB), SUB)
        q = queries[side, :, t * TILE : (t + 1) * TILE]
        s = jnp.dot(kv[at, 0:width], q, preferred_element_type=F32)
        scores[slot, i * SUB : (i + 1) * SUB] = s
        return jnp.max(s.reshape(SUB // 8, 8, TILE), axis=0)

    def score_all(chunk, side, t, slot):
        best = None
        for i in range(CHUNK // SUB):
            m = score(chunk, side, t, slot, i)
            best = m if best is None else jnp.maximum(best, m)
        peak[slot] = best

    n_steps = 2 * 4 * RING

    def chunk_of(s):
        mid, end = (s + 22) // 32, (s + 8) // 32
        return (1 - mid) * lax.rem(s, 5) + (mid - end) * (s // 2) + end * (12 + lax.rem(s, 4))

    def side_of(s):
        mid, end = (s + 22) // 32, (s + 8) // 32
        return (1 - mid) * (s // 5) + (mid - end) * lax.rem(s, 2) + end * (1 - lax.rem(s // 4, 2))

    turn(0, 0)
    score_all(0, 0, 0, 0)
    score_all(0, 0, 1, 1)

    def finish(side):
        flat = [acc[side, t] for t in range(n_tiles)]
        sums = jnp.concatenate([f[width : width + 8] for f in flat], axis=1)
        tops = jnp.concatenate([top[side, t] for t in range(n_tiles)], axis=1)
        outs = jnp.concatenate([f[0:width] / f[width : width + 1] for f in flat], axis=1)
        logs = (tops + jnp.log2(sums)) * LN2
        turned = jnp.transpose(jnp.concatenate([outs, logs], axis=0))
        for q in range(2):
            p = 2 * side + q
            for h in range(heads):
                base = (q * heads + h) * rows
                att[p, :, h * width : (h + 1) * width] = turned[base : base + rows, 0:width].astype(BF16)
        return turned

    def keep_logs(side, turned):
        for q in range(2):
            for h in range(heads):
                for i in range(2):
                    base = (q * heads + h) * rows + i * half
                    to = pl.ds(pl.multiple_of(starts[2 * side + q][i], half), half)
                    log_rows[to, h : h + 1] = turned[base : base + half, width : width + 1]

    def att_copy(p, i, source, at, slot, where):
        src = att.at[p] if i is None else att.at[p, part(i)]
        dst = att_in.at[source] if at is None else att_in.at[source, part(at)]
        return send(src, dst, att_send.at[slot], att_recv.at[source, at or 0], where)

    att_late = [
        att_copy(3, None, 2, None, 0, to_opposite),
        att_copy(2, 0, 1, 1, 1, to_left),
        att_copy(2, 1, 0, 0, 2, to_right),
    ]
    att_last = [att_copy(1, 0, 1, 0, 3, to_left), att_copy(1, 1, 0, 1, 4, to_right)]

    def at_step(s, now, acts):
        @pl.when(s == now)
        def _():
            for act in acts:
                act()

    def wait_tokens(p):
        for i in range(2):
            token_wait(p, i)

    def wo_one():
        wo_copy(1, 1, 0, 4, to_right).wait_recv()
        wo_on[0].start()
        wo_copy(2, 2, 1, 5, to_left).wait_recv()
        wo_on[1].start()

    def wo_two():
        for copy, block in zip(wo_rest, (1, 2)):
            copy.wait_recv()
            pair_copy(block).start()

    def wo_three():
        for copy in wo_on:
            copy.wait_recv()
        pair_copy(3).start()

    def wo_swap(*blocks):
        for block in blocks:
            pair_copy(block).wait_recv()
            wo_hand(block).start()

    def close_late():
        keep_logs(1, finish(1))
        for copy in att_late:
            copy.start()

    def later(f, *args):
        return functools.partial(f, *args)

    duties = {
        0: [later(from_mate, 0, 1)],
        1: [later(from_mate, 0, 3), later(wait_tokens, 2), later(piece_work, 2)],
        2: [later(hand, 0), later(spread, 1), later(from_mate, 0, 2)],
        3: [later(from_mate, 1, 0)],
        4: [later(wait_tokens, 3), later(piece_work, 3), later(relay, 1)],
        5: [later(spread, 2)],
        8: [later(hand, 1)],
        9: [later(from_mate, 1, 1)],
        10: [later(relay, 2)],
        11: [later(from_mate, 1, 3)],
        12: [later(spread, 3)],
        13: [later(from_mate, 1, 2), wo_one],
        15: [later(from_mate, 2, 0)],
        16: [later(hand, 2)],
        17: [later(from_mate, 2, 1)],
        18: [wo_two],
        19: [later(from_mate, 2, 3)],
        20: [later(relay, 3)],
        21: [later(from_mate, 2, 2)],
        22: [wo_three],
        23: [later(from_mate, 3, 0)],
        24: [later(from_mate, 3, 1)],
        25: [later(from_mate, 3, 3)],
        26: [later(hand, 3), later(wo_swap, 1, 2), later(from_mate, 3, 2)],
        28: [close_late],
        29: [later(wo_swap, 3)],
    }

    def step(s, carry):
        for now, acts in duties.items():
            if acts:
                at_step(s, now, acts)
        slot_v = lax.rem(s, 2)
        after = lax.rem(s + 1, n_steps)
        chunk, side = chunk_of(s), side_of(s)
        next_chunk, next_side = chunk_of(after), side_of(after)
        for t in range(n_tiles):
            if t == 1:
                turn(next_chunk, 1 - slot_v)
            ahead = t + 2
            to_chunk, to_side = (chunk, side) if ahead < n_tiles else (next_chunk, next_side)
            tile, fill, slot = ahead % n_tiles, ahead % 3, t % 3
            old = top[side, t]
            new = jnp.maximum(old, jnp.max(peak[slot], axis=0, keepdims=True))
            best = None
            total = None
            for i in range(CHUNK // SUB):
                m = score(to_chunk, to_side, tile, fill, i)
                best = m if best is None else jnp.maximum(best, m)
                at = slice(i * SUB, (i + 1) * SUB)
                weights = jnp.exp2(scores[slot, at] - new).astype(BF16)
                mixed = jnp.dot(turned_v[slot_v, :, at], weights, preferred_element_type=F32)
                total = mixed if total is None else total + mixed
            peak[fill] = best
            acc[side, t] = acc[side, t] * jnp.exp2(old - new) + total
            top[side, t] = new
        return carry

    lax.fori_loop(0, n_steps, step, 0)

    turned = finish(0)
    for copy in att_last:
        copy.start()
    keep_logs(0, turned)
    log_ref[...] = jnp.transpose(log_rows[...])[0:heads]

    for block in (1, 2, 3):
        other = wo_rows(block, 1 - core, 0, 4)
        send(other, other, wo_send.at[0], wo_recv.at[block, 3], to_mate).wait_recv()

    cols = 512

    def columns(n):
        return slice(n * cols, (n + 1) * cols)

    def times(x, block, n):
        return jnp.dot(x, wo[block, :, columns(n)], preferred_element_type=F32)

    att_late[0].wait_recv()
    for n in range(model // cols):
        product[:, columns(n)] = times(att[0], 0, n) + times(att_in[2], 3, n)
    for copy in att_late[1:] + att_last:
        copy.wait_recv()
    for n in range(model // cols):
        total = product[:, columns(n)] + times(att_in[0], 1, n) + times(att_in[1], 2, n)
        mixed_ref[:, columns(n)] = total.astype(BF16)

    for copy in token_out + token_on + wo_out + wo_on + att_late + att_last:
        copy.wait_send()
    for block in (1, 2, 3):
        pair_copy(block).wait_send()
        wo_hand(block).wait_send()
    for p in range(4):
        sent = kv.at[pl.ds(0, 31 * rows)]
        kv_copy(sent, sent, p, 0, core, to_mate).wait_send()


def body(tokens, query_weight, key_weight, value_weight, out_weight, query_gain, key_gain):
    rows, depth = tokens.shape
    query_cols = query_weight.shape[1]
    kv_cols = key_weight.shape[1]
    heads, width = query_gain.shape
    group, model = out_weight.shape
    count = rows * RING
    n_sp = RING * RING * 2
    n_tiles = 2 * heads * rows // TILE
    any_space = pl.BlockSpec(memory_space=pl.ANY)
    vmem = pl.BlockSpec(memory_space=pltpu.VMEM)
    dma = pltpu.SemaphoreType.DMA
    return pl.pallas_call(
        kernel,
        out_shape=(
            pltpu.VMEM((rows, model), BF16),
            pltpu.VMEM((heads, count), F32),
        ),
        in_specs=[any_space] * 5 + [vmem] * 2,
        out_specs=(vmem, vmem),
        scratch_shapes=[
            pltpu.VMEM((4, rows, depth), BF16),
            pltpu.VMEM((depth, query_cols), BF16),
            pltpu.VMEM((2 * kv_cols, depth), BF16),
            pltpu.VMEM((4, group, model), BF16),
            pltpu.VMEM((width, heads * rows + 128), F32),
            pltpu.VMEM((4, width, heads * rows), F32),
            pltpu.VMEM((2, width, 2 * heads * rows), BF16),
            pltpu.VMEM((n_sp * count, 2 * width), BF16),
            pltpu.VMEM((3, CHUNK, TILE), F32),
            pltpu.VMEM((3, 8, TILE), F32),
            pltpu.VMEM((2, width + ONES, CHUNK), BF16),
            pltpu.VMEM((2, n_tiles, width + ONES, TILE), F32),
            pltpu.VMEM((2, n_tiles, 1, TILE), F32),
            pltpu.VMEM((4, rows, group), BF16),
            pltpu.VMEM((3, rows, group), BF16),
            pltpu.VMEM((count, 128), F32),
            pltpu.VMEM((rows, model), F32),
            dma((5,)),
            dma((6,)),
            dma((4, 2)),
            dma((4,)),
            dma((4, RING, 2)),
            dma((12,)),
            dma((4, 4)),
            dma((5,)),
            dma((3, 2)),
        ],
        compiler_params=pltpu.CompilerParams(
            collective_id=0, has_side_effects=True, vmem_limit_bytes=60 * 1024 * 1024
        ),
        name="attention",
    )(tokens, query_weight, key_weight.T, value_weight.T, out_weight, query_gain, key_gain)


def solution(mesh):
    return jax.shard_map(
        body,
        mesh=mesh,
        in_specs=(
            P(("sp", "tp"), None),
            P(None, "tp"),
            P(None, "tp"),
            P(None, "tp"),
            P("tp", None),
            P("tp", None),
            P("tp", None),
        ),
        out_specs=(P(("sp", "tp"), None), P("tp", "sp")),
        check_vma=False,
    )
```

```python
import functools
import math

import jax
import jax.numpy as jnp
from jax import lax
from jax.experimental import pallas as pl
from jax.experimental.pallas import tpu as pltpu
from jax.sharding import PartitionSpec as P

GRID_W = 64
ROPE_BASE = 10000.0
EPS = 1e-06
LOG2E = math.log2(math.e)
LN2 = math.log(2.0)
ONES = 16
RING = 4
CHUNK = 768
TILE = 256
SUB = 256
MESH = pl.DeviceIdType.MESH
F32 = jnp.float32
BF16 = jnp.bfloat16


def prepare(x, gain, tables):
    quarter = x.shape[0] // 4
    x = x * lax.rsqrt(jnp.mean(x * x, axis=0, keepdims=True) + EPS) * gain
    a, b, c, d = (x[i * quarter : (i + 1) * quarter] for i in range(4))
    row_cos, row_sin, col_cos, col_sin = tables
    return jnp.concatenate(
        [
            a * row_cos - b * row_sin,
            b * row_cos + a * row_sin,
            c * col_cos - d * col_sin,
            d * col_cos + c * col_sin,
        ],
        axis=0,
    )


def kernel(
    tok_hbm,
    wq_hbm,
    wk_hbm,
    wv_hbm,
    wo_hbm,
    qg_ref,
    kg_ref,
    mixed_ref,
    log_ref,
    tok,
    wq,
    wkv,
    wo,
    gain_cols,
    tables,
    queries,
    kv,
    scores,
    peak,
    turned_v,
    acc,
    top,
    att,
    att_in,
    log_rows,
    product,
    local_sem,
    tok_send,
    tok_recv,
    kv_send,
    kv_recv,
    wo_send,
    wo_recv,
    att_send,
    att_recv,
):
    sp = lax.axis_index("sp")
    tp = lax.axis_index("tp")
    core = lax.rem(sp, 2)
    scores, peak, turned_v, acc, top, queries = (
        ref.at[core] for ref in (scores, peak, turned_v, acc, top, queries)
    )
    y = lax.rem(sp // 2, RING)
    z = sp // (2 * RING)
    mate = sp + 1 - 2 * core
    left, right, opposite = (lax.rem(tp + i, RING) for i in (3, 1, 2))
    rows = tok.shape[1]
    half = rows // 2
    heads, width = qg_ref.shape
    count = rows * RING
    kv_cols = wk_hbm.shape[0]
    group, model = wo_hbm.shape
    n_tiles = 2 * heads * rows // TILE

    coord_a = y * (1 - core) + z * core
    step_a = 2 + 6 * core
    coord_b = z * (1 - core) + y * core
    step_b = 8 - 6 * core

    def peer_a(i):
        return {"sp": sp + (lax.rem(coord_a + i, RING) - coord_a) * step_a}

    def peer_b(i):
        return {"sp": sp + (lax.rem(coord_b + i, RING) - coord_b) * step_b}

    loads = [
        pltpu.make_async_copy(src, dst, local_sem.at[i])
        for i, (src, dst) in enumerate(
            (
                (tok_hbm, tok.at[0]),
                (wk_hbm, wkv.at[0:kv_cols]),
                (wv_hbm, wkv.at[kv_cols:]),
                (wq_hbm, wq),
                (wo_hbm, wo.at[0]),
            )
        )
    ]
    for load in loads:
        load.start()

    barrier = pltpu.get_barrier_semaphore()
    for i in range(1, RING):
        pl.semaphore_signal(barrier, inc=1, device_id={"tp": lax.rem(tp + i, RING)}, device_id_type=MESH)
        pl.semaphore_signal(barrier, inc=1, device_id=peer_a(i), device_id_type=MESH)
        pl.semaphore_signal(barrier, inc=1, device_id=peer_b(i), device_id_type=MESH)
    pl.semaphore_signal(barrier, inc=1, device_id={"sp": mate}, device_id_type=MESH)
    pl.semaphore_wait(barrier, 3 * (RING - 1) + 1)

    def send(src, dst, send_sem, recv_sem, where):
        return pltpu.make_async_remote_copy(
            src_ref=src,
            dst_ref=dst,
            send_sem=send_sem,
            recv_sem=recv_sem,
            device_id=where,
            device_id_type=MESH,
        )

    def part(i):
        return slice(i * half, (i + 1) * half)

    to_left, to_right, to_opposite, to_mate = {"tp": left}, {"tp": right}, {"tp": opposite}, {"sp": mate}

    def token_copy(src, piece, i, slot, where):
        return send(src, tok.at[piece, part(i)], tok_send.at[slot], tok_recv.at[piece, i], where)

    first_half, second_half = tok_hbm.at[part(0)], tok_hbm.at[part(1)]
    token_out = [
        token_copy(first_half, 1, 0, 0, to_right),
        token_copy(second_half, 1, 1, 1, to_left),
        token_copy(second_half, 2, 0, 2, to_right),
        token_copy(first_half, 2, 1, 3, to_left),
    ]
    token_on = [
        token_copy(tok.at[1, part(0)], 3, 0, 4, to_right),
        token_copy(tok.at[1, part(1)], 3, 1, 5, to_left),
    ]
    for copy in token_out:
        copy.start()

    def token_wait(piece, i):
        token_copy(tok.at[1, part(i)], piece, i, 4 + i, to_right).wait_recv()

    starts = (
        (tp * rows, tp * rows + half),
        (left * rows, right * rows + half),
        (left * rows + half, right * rows),
        (opposite * rows, opposite * rows + half),
    )

    quarter = width // 4
    lane = lax.broadcasted_iota(jnp.int32, (quarter, heads * rows), 1)
    spot = lane
    for h in range(1, heads):
        spot = spot - jnp.where(lane >= h * rows, rows, 0)
    order = lax.broadcasted_iota(jnp.int32, (quarter, heads * rows), 0).astype(F32)
    freq = jnp.exp(order * (-math.log(ROPE_BASE) / quarter))
    shift = GRID_W.bit_length() - 1
    for p in range(4):
        a, b = starts[p]
        place = sp * count + spot + jnp.where(spot < half, a, b - half)
        row = lax.shift_right_logical(place, shift).astype(F32) * freq
        col = jnp.bitwise_and(place, GRID_W - 1).astype(F32) * freq
        tables[p, 0:quarter] = jnp.cos(row)
        tables[p, quarter : 2 * quarter] = jnp.sin(row)
        tables[p, 2 * quarter : 3 * quarter] = jnp.cos(col)
        tables[p, 3 * quarter :] = jnp.sin(col)

    gain_rows = [
        jnp.broadcast_to(qg_ref[h : h + 1, :].astype(F32) * (LOG2E * width ** (-0.5)), (rows, width))
        for h in range(heads)
    ]
    gain_rows.append(jnp.broadcast_to(kg_ref[...].astype(F32), (128, width)))
    gain_cols[...] = jnp.transpose(jnp.concatenate(gain_rows, axis=0))
    top[...] = jnp.full_like(top, -1e30)
    acc[...] = jnp.zeros_like(acc)
    turned_v[:, width:, :] = jnp.ones_like(turned_v[:, width:, :])
    log_rows[...] = jnp.zeros_like(log_rows)

    place_of = (0, 1, 3, 2)

    def kv_rows(p, shift, c, k, n):
        base = (((p * RING + place_of[shift]) * 2 + c) * RING + k) * rows
        return kv.at[pl.ds(pl.multiple_of(base, half), n)]

    def tables_of(p, n):
        return [tables[p, i * quarter : (i + 1) * quarter, 0:n] for i in range(4)]

    def make_kv(p):
        raw = lax.dot_general(tok[p], wkv[...], (((1,), (1,)), ((), ())), preferred_element_type=F32)
        turned = jnp.transpose(raw)
        gain = gain_cols[:, heads * rows : heads * rows + rows]
        keys = prepare(turned[0:width], gain, tables_of(p, rows))
        to = kv_rows(p, 0, core, 0, rows)
        to[:, 0:width] = jnp.transpose(keys).astype(BF16)
        to[:, width : 2 * width] = raw[:, width:].astype(BF16)

    def make_queries(p):
        raw = jnp.dot(tok[p], wq[...], preferred_element_type=F32)
        stacked = jnp.concatenate([raw[:, h * width : (h + 1) * width] for h in range(heads)], axis=0)
        q = prepare(jnp.transpose(stacked), gain_cols[:, 0 : heads * rows], tables_of(p, heads * rows))
        at = slice((p % 2) * heads * rows, (p % 2 + 1) * heads * rows)
        queries[p // 2, :, at] = q.astype(BF16)

    def kv_copy(src, dst, p, shift, c, where):
        return send(src, dst, kv_send.at[p], kv_recv.at[p, place_of[shift], c], where)

    whole = RING * rows

    def own_send(p):
        src = kv_rows(p, 0, core, 0, rows)
        for i in (1, 3, 2):
            kv_copy(src, kv_rows(p, 0, core, RING - i, rows), p, 0, core, peer_a(i)).start()

    def hand_copy(p, shift):
        spot = kv_rows(p, shift, core, 0, whole)
        return kv_copy(spot, spot, p, shift, core, to_mate)

    def spread(p):
        spot = kv_rows(p, 0, core, 1, whole - rows)
        kv_copy(spot, spot, p, 0, core, to_mate).wait_recv()
        src = kv_rows(p, 0, core, 0, whole)
        for i in (1, 3):
            kv_copy(src, kv_rows(p, RING - i, core, 0, whole), p, RING - i, core, peer_b(i)).start()
        hand_copy(p, 0).start()

    def relay(p):
        for shift, k, to in ((3, 0, 1), (1, 2, 3)):
            hand_copy(p, shift).wait_recv()
            src = kv_rows(p, shift, core, k, 2 * rows)
            kv_copy(src, kv_rows(p, 2, core, k, 2 * rows), p, 2, core, peer_b(to)).start()
            hand_copy(p, shift).start()

    def hand(p):
        hand_copy(p, 2).wait_recv()
        hand_copy(p, 2).start()

    def from_mate(p, shift):
        spot = kv_rows(p, shift, 1 - core, 0, whole)
        kv_copy(spot, spot, p, shift, 1 - core, to_mate).wait_recv()

    strip = group // 8
    parity = lax.rem(coord_a, 2)
    to_pair = {"sp": sp + (1 - 2 * parity) * step_a}

    def wo_rows(block, side, first, n):
        return wo.at[block, pl.ds(pl.multiple_of((side * 4 + first) * strip, strip), n * strip)]

    def wo_copy(block, to_block, i, slot, where):
        at = 2 * parity + i
        return send(
            wo_rows(block, core, at, 1), wo_rows(to_block, core, at, 1), wo_send.at[slot], wo_recv.at[to_block, i], where
        )

    wo_out = [
        wo_copy(0, 1, 0, 0, to_right),
        wo_copy(0, 2, 1, 1, to_left),
        wo_copy(0, 1, 1, 2, to_right),
        wo_copy(0, 2, 0, 3, to_left),
    ]
    wo_on = [wo_copy(1, 3, 0, 4, to_right), wo_copy(2, 3, 1, 5, to_left)]
    wo_rest = [wo_copy(0, 1, 1, 2, to_right), wo_copy(0, 2, 0, 3, to_left)]

    def pair_copy(block):
        spot = wo_rows(block, core, 2 * parity, 2)
        return send(spot, spot, wo_send.at[5 + block], wo_recv.at[block, 2], to_pair)

    def wo_hand(block):
        spot = wo_rows(block, core, 0, 4)
        return send(spot, spot, wo_send.at[8 + block], wo_recv.at[block, 3], to_mate)

    def piece_work(p):
        make_kv(p)
        own_send(p)
        make_queries(p)

    loads[0].wait()
    loads[1].wait()
    loads[2].wait()
    make_kv(0)
    own_send(0)
    loads[3].wait()
    make_queries(0)
    spread(0)
    for i, copy in enumerate(token_on):
        token_wait(1, i)
        copy.start()
    loads[4].wait()
    for copy in wo_out:
        copy.start()
    piece_work(1)
    relay(0)
    from_mate(0, 0)

    def turn(chunk, slot):
        at = pl.ds(pl.multiple_of(chunk * CHUNK, CHUNK), CHUNK)
        turned_v[slot, 0:width] = jnp.transpose(kv[at])[width : 2 * width]

    def score(chunk, side, t, slot, i):
        at = pl.ds(pl.multiple_of(chunk * CHUNK + i * SUB, SUB), SUB)
        q = queries[side, :, t * TILE : (t + 1) * TILE]
        s = jnp.dot(kv[at, 0:width], q, preferred_element_type=F32)
        scores[slot, i * SUB : (i + 1) * SUB] = s
        return jnp.max(s.reshape(SUB // 8, 8, TILE), axis=0)

    def score_all(chunk, side, t, slot):
        best = None
        for i in range(CHUNK // SUB):
            m = score(chunk, side, t, slot, i)
            best = m if best is None else jnp.maximum(best, m)
        peak[slot] = best

    def finish(side):
        flat = [acc[side, t] for t in range(n_tiles)]
        sums = jnp.concatenate([f[width : width + 8] for f in flat], axis=1)
        tops = jnp.concatenate([top[side, t] for t in range(n_tiles)], axis=1)
        outs = jnp.concatenate([f[0:width] / f[width : width + 1] for f in flat], axis=1)
        logs = (tops + jnp.log2(sums)) * LN2
        turned = jnp.transpose(jnp.concatenate([outs, logs], axis=0))
        for q in range(2):
            p = 2 * side + q
            for h in range(heads):
                base = (q * heads + h) * rows
                att[p, :, h * width : (h + 1) * width] = turned[base : base + rows, 0:width].astype(BF16)
        return turned

    def keep_logs(side, turned):
        for q in range(2):
            for h in range(heads):
                for i in range(2):
                    base = (q * heads + h) * rows + i * half
                    to = pl.ds(pl.multiple_of(starts[2 * side + q][i], half), half)
                    log_rows[to, h : h + 1] = turned[base : base + half, width : width + 1]

    def att_copy(p, i, source, at, slot, where):
        src = att.at[p] if i is None else att.at[p, part(i)]
        dst = att_in.at[source] if at is None else att_in.at[source, part(at)]
        return send(src, dst, att_send.at[slot], att_recv.at[source, at or 0], where)

    att_late = [
        att_copy(3, None, 2, None, 0, to_opposite),
        att_copy(2, 0, 1, 1, 1, to_left),
        att_copy(2, 1, 0, 0, 2, to_right),
    ]
    att_last = [att_copy(1, 0, 1, 0, 3, to_left), att_copy(1, 1, 0, 1, 4, to_right)]

    def wait_tokens(p):
        for i in range(2):
            token_wait(p, i)

    def wo_one():
        wo_copy(1, 1, 0, 4, to_right).wait_recv()
        wo_on[0].start()
        wo_copy(2, 2, 1, 5, to_left).wait_recv()
        wo_on[1].start()

    def wo_two():
        for copy, block in zip(wo_rest, (1, 2)):
            copy.wait_recv()
            pair_copy(block).start()

    def wo_three():
        for copy in wo_on:
            copy.wait_recv()
        pair_copy(3).start()

    def wo_swap(*blocks):
        for block in blocks:
            pair_copy(block).wait_recv()
            wo_hand(block).start()

    def close_late():
        keep_logs(1, finish(1))
        for copy in att_late:
            copy.start()

    def items(side, *spots):
        return [(p * RING + place_of[shift], side) for p, shift in spots]

    def both(*spots):
        return [item for spot in spots for item in items(1, spot) + items(0, spot)]

    def attend(item, after, slot_v):
        chunk, side = item
        for t in range(n_tiles):
            ahead = t + 2
            target = item if ahead < n_tiles else after
            if t == 1 and after is not None:
                turn(after[0], 1 - slot_v)
            tile, fill, slot = ahead % n_tiles, ahead % 3, t % 3
            old = top[side, t]
            new = jnp.maximum(old, jnp.max(peak[slot], axis=0, keepdims=True))
            best = None
            total = None
            for i in range(CHUNK // SUB):
                if target is not None:
                    m = score(target[0], target[1], tile, fill, i)
                    best = m if best is None else jnp.maximum(best, m)
                at = slice(i * SUB, (i + 1) * SUB)
                weights = jnp.exp2(scores[slot, at] - new).astype(BF16)
                mixed = jnp.dot(turned_v[slot_v, :, at], weights, preferred_element_type=F32)
                total = mixed if total is None else total + mixed
            if target is not None:
                peak[fill] = best
            acc[side, t] = acc[side, t] * jnp.exp2(old - new) + total
            top[side, t] = new

    def run(todo, slot_v, after=None, cold=False):
        if cold:
            turn(todo[0][0], slot_v)
            for t in range(2):
                score_all(todo[0][0], todo[0][1], t, t)
        for n, item in enumerate(todo):
            attend(item, todo[n + 1] if n + 1 < len(todo) else after, (slot_v + n) % 2)
        return (slot_v + len(todo)) % 2

    def next_piece(p):
        wait_tokens(p)
        piece_work(p)

    def mates(*spots):
        for spot in spots:
            from_mate(*spot)

    next_piece(2)
    spread(1)
    mates((0, 1), (0, 3))
    run(items(0, (0, 0), (0, 1), (0, 3)), 0, cold=True)
    hand(0)
    from_mate(1, 0)
    run(items(0, (1, 0)), 0, cold=True)
    next_piece(3)
    relay(1)
    spread(2)
    from_mate(0, 2)
    plan = [
        items(1, (0, 0), (0, 1), (0, 3)),
        both((0, 2)) + items(1, (1, 0)),
        both((1, 1), (1, 3)),
        both((2, 0)) + items(1, (1, 2)),
        items(0, (1, 2)) + both((2, 1)) + items(1, (2, 3)),
        items(0, (2, 3)) + items(1, (3, 0)),
        items(0, (3, 0)) + both((2, 2)) + items(1, (3, 1)),
        items(0, (3, 1)) + items(1, (3, 3)),
        items(0, (3, 3)) + items(1, (3, 2)),
        items(0, (3, 2)),
    ]

    def before(n):
        if n == 1:
            from_mate(1, 1)
        if n == 2:
            hand(1)
            mates((1, 3), (2, 0))
        if n == 3:
            relay(2)
            spread(3)
            wo_one()
            from_mate(1, 2)
        if n == 4:
            wo_two()
            mates((2, 1), (2, 3))
        if n == 5:
            hand(2)
            relay(3)
            from_mate(3, 0)
        if n == 6:
            wo_three()
            mates((2, 2), (3, 1))
        if n == 7:
            hand(3)
            wo_swap(1, 2)
            from_mate(3, 3)
        if n == 8:
            wo_swap(3)
            from_mate(3, 2)
        if n == 9:
            close_late()

    slot_v = 0
    for n, todo in enumerate(plan):
        before(n)
        slot_v = run(todo, slot_v, plan[n + 1][0] if n + 1 < len(plan) else None, cold=n == 0)

    turned = finish(0)
    for copy in att_last:
        copy.start()
    keep_logs(0, turned)
    log_ref[...] = jnp.transpose(log_rows[...])[0:heads]

    for block in (1, 2, 3):
        other = wo_rows(block, 1 - core, 0, 4)
        send(other, other, wo_send.at[0], wo_recv.at[block, 3], to_mate).wait_recv()

    cols = 512

    def columns(n):
        return slice(n * cols, (n + 1) * cols)

    def times(x, block, n):
        return jnp.dot(x, wo[block, :, columns(n)], preferred_element_type=F32)

    att_late[0].wait_recv()
    for n in range(model // cols):
        product[:, columns(n)] = times(att[0], 0, n) + times(att_in[2], 3, n)
    for copy in att_late[1:] + att_last:
        copy.wait_recv()
    for n in range(model // cols):
        total = product[:, columns(n)] + times(att_in[0], 1, n) + times(att_in[1], 2, n)
        mixed_ref[:, columns(n)] = total.astype(BF16)

    for copy in token_out + token_on + wo_out + wo_on + att_late + att_last:
        copy.wait_send()
    for block in (1, 2, 3):
        pair_copy(block).wait_send()
        wo_hand(block).wait_send()
    for p in range(4):
        sent = kv.at[pl.ds(0, 31 * rows)]
        kv_copy(sent, sent, p, 0, core, to_mate).wait_send()


def body(tokens, query_weight, key_weight, value_weight, out_weight, query_gain, key_gain):
    rows, depth = tokens.shape
    query_cols = query_weight.shape[1]
    kv_cols = key_weight.shape[1]
    heads, width = query_gain.shape
    group, model = out_weight.shape
    count = rows * RING
    n_sp = RING * RING * 2
    n_tiles = 2 * heads * rows // TILE
    any_space = pl.BlockSpec(memory_space=pl.ANY)
    vmem = pl.BlockSpec(memory_space=pltpu.VMEM)
    dma = pltpu.SemaphoreType.DMA
    return pl.pallas_call(
        kernel,
        out_shape=(
            pltpu.VMEM((rows, model), BF16),
            pltpu.VMEM((heads, count), F32),
        ),
        in_specs=[any_space] * 5 + [vmem] * 2,
        out_specs=(vmem, vmem),
        scratch_shapes=[
            pltpu.VMEM((4, rows, depth), BF16),
            pltpu.VMEM((depth, query_cols), BF16),
            pltpu.VMEM((2 * kv_cols, depth), BF16),
            pltpu.VMEM((4, group, model), BF16),
            pltpu.VMEM((width, heads * rows + 128), F32),
            pltpu.VMEM((4, width, heads * rows), F32),
            pltpu.VMEM((2, 2, width, 2 * heads * rows), BF16),
            pltpu.VMEM((n_sp * count, 2 * width), BF16),
            pltpu.VMEM((2, 3, CHUNK, TILE), F32),
            pltpu.VMEM((2, 3, 8, TILE), F32),
            pltpu.VMEM((2, 2, width + ONES, CHUNK), BF16),
            pltpu.VMEM((2, 2, n_tiles, width + ONES, TILE), F32),
            pltpu.VMEM((2, 2, n_tiles, 1, TILE), F32),
            pltpu.VMEM((4, rows, group), BF16),
            pltpu.VMEM((3, rows, group), BF16),
            pltpu.VMEM((count, 128), F32),
            pltpu.VMEM((rows, model), F32),
            dma((5,)),
            dma((6,)),
            dma((4, 2)),
            dma((4,)),
            dma((4, RING, 2)),
            dma((12,)),
            dma((4, 4)),
            dma((5,)),
            dma((3, 2)),
        ],
        compiler_params=pltpu.CompilerParams(
            collective_id=0, has_side_effects=True, vmem_limit_bytes=60 * 1024 * 1024
        ),
        name="attention",
    )(tokens, query_weight, key_weight.T, value_weight.T, out_weight, query_gain, key_gain)


def solution(mesh):
    return jax.shard_map(
        body,
        mesh=mesh,
        in_specs=(
            P(("sp", "tp"), None),
            P(None, "tp"),
            P(None, "tp"),
            P(None, "tp"),
            P("tp", None),
            P("tp", None),
            P("tp", None),
        ),
        out_specs=(P(("sp", "tp"), None), P("tp", "sp")),
        check_vma=False,
    )
```

```python
import functools
import math

import jax
import jax.numpy as jnp
from jax import lax
from jax.experimental import pallas as pl
from jax.experimental.pallas import tpu as pltpu
from jax.sharding import PartitionSpec as P

GRID_W = 64
ROPE_BASE = 10000.0
EPS = 1e-06
LOG2E = math.log2(math.e)
LN2 = math.log(2.0)
ONES = 16
RING = 4
CHUNK = 768
TILE = 256
SUB = 256
MESH = pl.DeviceIdType.MESH
F32 = jnp.float32
BF16 = jnp.bfloat16


def prepare(x, gain, tables):
    quarter = x.shape[0] // 4
    x = x * lax.rsqrt(jnp.mean(x * x, axis=0, keepdims=True) + EPS) * gain
    a, b, c, d = (x[i * quarter : (i + 1) * quarter] for i in range(4))
    row_cos, row_sin, col_cos, col_sin = tables
    return jnp.concatenate(
        [
            a * row_cos - b * row_sin,
            b * row_cos + a * row_sin,
            c * col_cos - d * col_sin,
            d * col_cos + c * col_sin,
        ],
        axis=0,
    )


def kernel(
    tok_hbm,
    wq_hbm,
    wk_hbm,
    wv_hbm,
    wo_hbm,
    qg_ref,
    kg_ref,
    mixed_ref,
    log_ref,
    tok,
    wq,
    wkv,
    wo,
    gain_cols,
    tables,
    queries,
    kv,
    scores,
    peak,
    turned_v,
    acc,
    top,
    att,
    att_in,
    log_rows,
    product,
    local_sem,
    tok_send,
    tok_recv,
    kv_send,
    kv_recv,
    wo_send,
    wo_recv,
    att_send,
    att_recv,
):
    sp = lax.axis_index("sp")
    tp = lax.axis_index("tp")
    core = lax.rem(sp, 2)
    scores, peak, turned_v, acc, top, queries = (
        ref.at[core] for ref in (scores, peak, turned_v, acc, top, queries)
    )
    y = lax.rem(sp // 2, RING)
    z = sp // (2 * RING)
    mate = sp + 1 - 2 * core
    left, right, opposite = (lax.rem(tp + i, RING) for i in (3, 1, 2))
    rows = tok.shape[1]
    half = rows // 2
    heads, width = qg_ref.shape
    count = rows * RING
    kv_cols = wk_hbm.shape[0]
    group, model = wo_hbm.shape
    n_tiles = 2 * heads * rows // TILE

    coord_a = y * (1 - core) + z * core
    step_a = 2 + 6 * core
    coord_b = z * (1 - core) + y * core
    step_b = 8 - 6 * core

    def peer_a(i):
        return {"sp": sp + (lax.rem(coord_a + i, RING) - coord_a) * step_a}

    def peer_b(i):
        return {"sp": sp + (lax.rem(coord_b + i, RING) - coord_b) * step_b}

    loads = [
        pltpu.make_async_copy(src, dst, local_sem.at[i])
        for i, (src, dst) in enumerate(
            (
                (tok_hbm, tok.at[0]),
                (wk_hbm, wkv.at[0:kv_cols]),
                (wv_hbm, wkv.at[kv_cols:]),
                (wq_hbm, wq),
                (wo_hbm, wo.at[0]),
            )
        )
    ]
    for load in loads:
        load.start()

    barrier = pltpu.get_barrier_semaphore()
    for i in range(1, RING):
        pl.semaphore_signal(barrier, inc=1, device_id={"tp": lax.rem(tp + i, RING)}, device_id_type=MESH)
        pl.semaphore_signal(barrier, inc=1, device_id=peer_a(i), device_id_type=MESH)
        pl.semaphore_signal(barrier, inc=1, device_id=peer_b(i), device_id_type=MESH)
    pl.semaphore_signal(barrier, inc=1, device_id={"sp": mate}, device_id_type=MESH)
    pl.semaphore_wait(barrier, 3 * (RING - 1) + 1)

    def send(src, dst, send_sem, recv_sem, where):
        return pltpu.make_async_remote_copy(
            src_ref=src,
            dst_ref=dst,
            send_sem=send_sem,
            recv_sem=recv_sem,
            device_id=where,
            device_id_type=MESH,
        )

    def part(i):
        return slice(i * half, (i + 1) * half)

    to_left, to_right, to_opposite, to_mate = {"tp": left}, {"tp": right}, {"tp": opposite}, {"sp": mate}

    def token_copy(src, piece, i, slot, where):
        return send(src, tok.at[piece, part(i)], tok_send.at[slot], tok_recv.at[piece, i], where)

    first_half, second_half = tok_hbm.at[part(0)], tok_hbm.at[part(1)]
    token_out = [
        token_copy(first_half, 1, 0, 0, to_right),
        token_copy(second_half, 1, 1, 1, to_left),
        token_copy(second_half, 2, 0, 2, to_right),
        token_copy(first_half, 2, 1, 3, to_left),
    ]
    token_on = [
        token_copy(tok.at[1, part(0)], 3, 0, 4, to_right),
        token_copy(tok.at[1, part(1)], 3, 1, 5, to_left),
    ]
    for copy in token_out:
        copy.start()

    def token_wait(piece, i):
        token_copy(tok.at[1, part(i)], piece, i, 4 + i, to_right).wait_recv()

    starts = (
        (tp * rows, tp * rows + half),
        (left * rows, right * rows + half),
        (left * rows + half, right * rows),
        (opposite * rows, opposite * rows + half),
    )

    quarter = width // 4
    lane = lax.broadcasted_iota(jnp.int32, (quarter, heads * rows), 1)
    spot = lane
    for h in range(1, heads):
        spot = spot - jnp.where(lane >= h * rows, rows, 0)
    order = lax.broadcasted_iota(jnp.int32, (quarter, heads * rows), 0).astype(F32)
    freq = jnp.exp(order * (-math.log(ROPE_BASE) / quarter))
    shift = GRID_W.bit_length() - 1
    for p in range(4):
        a, b = starts[p]
        place = sp * count + spot + jnp.where(spot < half, a, b - half)
        row = lax.shift_right_logical(place, shift).astype(F32) * freq
        col = jnp.bitwise_and(place, GRID_W - 1).astype(F32) * freq
        tables[p, 0:quarter] = jnp.cos(row)
        tables[p, quarter : 2 * quarter] = jnp.sin(row)
        tables[p, 2 * quarter : 3 * quarter] = jnp.cos(col)
        tables[p, 3 * quarter :] = jnp.sin(col)

    gain_rows = [
        jnp.broadcast_to(qg_ref[h : h + 1, :].astype(F32) * (LOG2E * width ** (-0.5)), (rows, width))
        for h in range(heads)
    ]
    gain_rows.append(jnp.broadcast_to(kg_ref[...].astype(F32), (128, width)))
    gain_cols[...] = jnp.transpose(jnp.concatenate(gain_rows, axis=0))
    top[...] = jnp.full_like(top, -1e30)
    acc[...] = jnp.zeros_like(acc)
    turned_v[:, width:, :] = jnp.ones_like(turned_v[:, width:, :])
    log_rows[...] = jnp.zeros_like(log_rows)

    place_of = (0, 1, 3, 2)

    def kv_rows(p, shift, c, k, n):
        base = (((p * RING + place_of[shift]) * 2 + c) * RING + k) * rows
        return kv.at[pl.ds(pl.multiple_of(base, half), n)]

    def tables_of(p, n):
        return [tables[p, i * quarter : (i + 1) * quarter, 0:n] for i in range(4)]

    def make_kv(p):
        raw = lax.dot_general(tok[p], wkv[...], (((1,), (1,)), ((), ())), preferred_element_type=F32)
        turned = jnp.transpose(raw)
        gain = gain_cols[:, heads * rows : heads * rows + rows]
        keys = prepare(turned[0:width], gain, tables_of(p, rows))
        to = kv_rows(p, 0, core, 0, rows)
        to[:, 0:width] = jnp.transpose(keys).astype(BF16)
        to[:, width : 2 * width] = raw[:, width:].astype(BF16)

    def make_queries(p):
        raw = jnp.dot(tok[p], wq[...], preferred_element_type=F32)
        stacked = jnp.concatenate([raw[:, h * width : (h + 1) * width] for h in range(heads)], axis=0)
        q = prepare(jnp.transpose(stacked), gain_cols[:, 0 : heads * rows], tables_of(p, heads * rows))
        at = slice((p % 2) * heads * rows, (p % 2 + 1) * heads * rows)
        queries[p // 2, :, at] = q.astype(BF16)

    def kv_copy(src, dst, p, shift, c, where):
        return send(src, dst, kv_send.at[p], kv_recv.at[p, place_of[shift], c], where)

    whole = RING * rows

    def own_send(p):
        src = kv_rows(p, 0, core, 0, rows)
        for i in (1, 3, 2):
            kv_copy(src, kv_rows(p, 0, core, RING - i, rows), p, 0, core, peer_a(i)).start()

    def hand_copy(p, shift):
        spot = kv_rows(p, shift, core, 0, whole)
        return kv_copy(spot, spot, p, shift, core, to_mate)

    def spread(p):
        spot = kv_rows(p, 0, core, 1, whole - rows)
        kv_copy(spot, spot, p, 0, core, to_mate).wait_recv()
        src = kv_rows(p, 0, core, 0, whole)
        for i in (1, 3):
            kv_copy(src, kv_rows(p, RING - i, core, 0, whole), p, RING - i, core, peer_b(i)).start()
        hand_copy(p, 0).start()

    def relay(p):
        for shift, k, to in ((3, 0, 1), (1, 2, 3)):
            hand_copy(p, shift).wait_recv()
            src = kv_rows(p, shift, core, k, 2 * rows)
            kv_copy(src, kv_rows(p, 2, core, k, 2 * rows), p, 2, core, peer_b(to)).start()
            hand_copy(p, shift).start()

    def hand(p):
        hand_copy(p, 2).wait_recv()
        hand_copy(p, 2).start()

    def from_mate(p, shift):
        spot = kv_rows(p, shift, 1 - core, 0, whole)
        kv_copy(spot, spot, p, shift, 1 - core, to_mate).wait_recv()

    strip = group // 8
    parity = lax.rem(coord_a, 2)
    to_pair = {"sp": sp + (1 - 2 * parity) * step_a}

    def wo_rows(block, side, first, n):
        return wo.at[block, pl.ds(pl.multiple_of((side * 4 + first) * strip, strip), n * strip)]

    def wo_copy(block, to_block, i, slot, where):
        at = 2 * parity + i
        return send(
            wo_rows(block, core, at, 1), wo_rows(to_block, core, at, 1), wo_send.at[slot], wo_recv.at[to_block, i], where
        )

    wo_out = [
        wo_copy(0, 1, 0, 0, to_right),
        wo_copy(0, 2, 1, 1, to_left),
        wo_copy(0, 1, 1, 2, to_right),
        wo_copy(0, 2, 0, 3, to_left),
    ]
    wo_on = [wo_copy(1, 3, 0, 4, to_right), wo_copy(2, 3, 1, 5, to_left)]
    wo_rest = [wo_copy(0, 1, 1, 2, to_right), wo_copy(0, 2, 0, 3, to_left)]

    def pair_copy(block):
        spot = wo_rows(block, core, 2 * parity, 2)
        return send(spot, spot, wo_send.at[5 + block], wo_recv.at[block, 2], to_pair)

    def wo_hand(block):
        spot = wo_rows(block, core, 0, 4)
        return send(spot, spot, wo_send.at[8 + block], wo_recv.at[block, 3], to_mate)

    def piece_work(p):
        make_kv(p)
        own_send(p)
        make_queries(p)

    loads[0].wait()
    loads[1].wait()
    loads[2].wait()
    make_kv(0)
    own_send(0)
    loads[3].wait()
    make_queries(0)
    spread(0)
    for i, copy in enumerate(token_on):
        token_wait(1, i)
        copy.start()
    loads[4].wait()
    for copy in wo_out:
        copy.start()
    piece_work(1)
    relay(0)
    from_mate(0, 0)

    def turn(chunk, slot):
        at = pl.ds(pl.multiple_of(chunk * CHUNK, CHUNK), CHUNK)
        turned_v[slot, 0:width] = jnp.transpose(kv[at])[width : 2 * width]

    def score(chunk, side, t, slot, i):
        at = pl.ds(pl.multiple_of(chunk * CHUNK + i * SUB, SUB), SUB)
        q = queries[side, :, t * TILE : (t + 1) * TILE]
        s = jnp.dot(kv[at, 0:width], q, preferred_element_type=F32)
        scores[slot, i * SUB : (i + 1) * SUB] = s
        return jnp.max(s.reshape(SUB // 8, 8, TILE), axis=0)

    def score_all(chunk, side, t, slot):
        best = None
        for i in range(CHUNK // SUB):
            m = score(chunk, side, t, slot, i)
            best = m if best is None else jnp.maximum(best, m)
        peak[slot] = best

    def finish(side):
        flat = [acc[side, t] for t in range(n_tiles)]
        sums = jnp.concatenate([f[width : width + 8] for f in flat], axis=1)
        tops = jnp.concatenate([top[side, t] for t in range(n_tiles)], axis=1)
        outs = jnp.concatenate([f[0:width] / f[width : width + 1] for f in flat], axis=1)
        logs = (tops + jnp.log2(sums)) * LN2
        turned = jnp.transpose(jnp.concatenate([outs, logs], axis=0))
        for q in range(2):
            p = 2 * side + q
            for h in range(heads):
                base = (q * heads + h) * rows
                att[p, :, h * width : (h + 1) * width] = turned[base : base + rows, 0:width].astype(BF16)
        return turned

    def keep_logs(side, turned):
        for q in range(2):
            for h in range(heads):
                for i in range(2):
                    base = (q * heads + h) * rows + i * half
                    to = pl.ds(pl.multiple_of(starts[2 * side + q][i], half), half)
                    log_rows[to, h : h + 1] = turned[base : base + half, width : width + 1]

    def att_copy(p, i, source, at, slot, where):
        src = att.at[p] if i is None else att.at[p, part(i)]
        dst = att_in.at[source] if at is None else att_in.at[source, part(at)]
        return send(src, dst, att_send.at[slot], att_recv.at[source, at or 0], where)

    att_late = [
        att_copy(3, None, 2, None, 0, to_opposite),
        att_copy(2, 0, 1, 1, 1, to_left),
        att_copy(2, 1, 0, 0, 2, to_right),
    ]
    att_last = [att_copy(1, 0, 1, 0, 3, to_left), att_copy(1, 1, 0, 1, 4, to_right)]

    def wait_tokens(p):
        for i in range(2):
            token_wait(p, i)

    def wo_one():
        wo_copy(1, 1, 0, 4, to_right).wait_recv()
        wo_on[0].start()
        wo_copy(2, 2, 1, 5, to_left).wait_recv()
        wo_on[1].start()

    def wo_two():
        for copy, block in zip(wo_rest, (1, 2)):
            copy.wait_recv()
            pair_copy(block).start()

    def wo_three():
        for copy in wo_on:
            copy.wait_recv()
        pair_copy(3).start()

    def wo_swap(*blocks):
        for block in blocks:
            pair_copy(block).wait_recv()
            wo_hand(block).start()

    def close_late():
        keep_logs(1, finish(1))
        for copy in att_late:
            copy.start()

    def items(side, *spots):
        return [(p * RING + place_of[shift], side) for p, shift in spots]

    def both(*spots):
        return [item for spot in spots for item in items(1, spot) + items(0, spot)]

    def attend(item, after, slot_v):
        chunk, side = item
        for t in range(n_tiles):
            ahead = t + 2
            target = item if ahead < n_tiles else after
            if t == 1 and after is not None:
                turn(after[0], 1 - slot_v)
            tile, fill, slot = ahead % n_tiles, ahead % 3, t % 3
            old = top[side, t]
            new = jnp.maximum(old, jnp.max(peak[slot], axis=0, keepdims=True))
            best = None
            total = None
            for i in range(CHUNK // SUB):
                if target is not None:
                    m = score(target[0], target[1], tile, fill, i)
                    best = m if best is None else jnp.maximum(best, m)
                at = slice(i * SUB, (i + 1) * SUB)
                weights = jnp.exp2(scores[slot, at] - new).astype(BF16)
                mixed = jnp.dot(turned_v[slot_v, :, at], weights, preferred_element_type=F32)
                total = mixed if total is None else total + mixed
            if target is not None:
                peak[fill] = best
            acc[side, t] = acc[side, t] * jnp.exp2(old - new) + total
            top[side, t] = new

    def run(todo, slot_v, after=None, cold=False):
        if cold:
            turn(todo[0][0], slot_v)
            for t in range(2):
                score_all(todo[0][0], todo[0][1], t, t)
        for n, item in enumerate(todo):
            attend(item, todo[n + 1] if n + 1 < len(todo) else after, (slot_v + n) % 2)
        return (slot_v + len(todo)) % 2

    def next_piece(p):
        wait_tokens(p)
        piece_work(p)

    def mates(*spots):
        for spot in spots:
            from_mate(*spot)

    next_piece(2)
    spread(1)
    mates((0, 1), (0, 3))
    run(items(0, (0, 0), (0, 1), (0, 3)), 0, cold=True)
    hand(0)
    from_mate(1, 0)
    run(items(0, (1, 0)), 0, cold=True)
    next_piece(3)
    relay(1)
    spread(2)
    from_mate(0, 2)
    plan = [
        items(1, (0, 0), (0, 1), (0, 3)),
        both((0, 2)) + items(1, (1, 0)),
        both((1, 1)),
        both((1, 3)) + items(1, (2, 0)),
        items(0, (2, 0)) + both((1, 2)),
        both((2, 1)) + items(1, (2, 3)),
        items(0, (2, 3)) + both((3, 0)) + items(1, (3, 1)),
        items(0, (3, 1)) + items(1, (2, 2)),
        items(0, (2, 2)) + items(1, (3, 3)),
        items(0, (3, 3)) + items(1, (3, 2)),
        items(0, (3, 2)),
    ]

    def before(n):
        if n == 1:
            from_mate(1, 1)
        if n == 2:
            spread(3)
            hand(1)
            wo_one()
            mates((1, 3), (2, 0))
        if n == 3:
            relay(2)
        if n == 4:
            wo_two()
            mates((1, 2), (2, 1))
        if n == 5:
            relay(3)
            from_mate(2, 3)
        if n == 6:
            hand(2)
            wo_three()
            mates((3, 0), (3, 1))
        if n == 7:
            from_mate(2, 2)
        if n == 8:
            hand(3)
            from_mate(3, 3)
        if n == 9:
            from_mate(3, 2)
        if n == 10:
            close_late()

    slot_v = 0
    for n, todo in enumerate(plan):
        before(n)
        slot_v = run(todo, slot_v, plan[n + 1][0] if n + 1 < len(plan) else None, cold=n == 0)

    turned = finish(0)
    for copy in att_last:
        copy.start()
    keep_logs(0, turned)
    log_ref[...] = jnp.transpose(log_rows[...])[0:heads]

    wo_swap(1, 2, 3)

    cols = 512

    def columns(n):
        return slice(n * cols, (n + 1) * cols)

    def times(x, block, n):
        return jnp.dot(x, wo[block, :, columns(n)], preferred_element_type=F32)

    for n in range(model // cols):
        product[:, columns(n)] = times(att[0], 0, n)
    for copy in token_out + token_on + wo_out + wo_on:
        copy.wait_send()
    for p in range(4):
        sent = kv.at[pl.ds(0, 31 * rows)]
        kv_copy(sent, sent, p, 0, core, to_mate).wait_send()
    for block in (1, 2, 3):
        pair_copy(block).wait_send()
        wo_hand(block).wait_send()
        other = wo_rows(block, 1 - core, 0, 4)
        send(other, other, wo_send.at[0], wo_recv.at[block, 3], to_mate).wait_recv()
    for copy in att_late + att_last:
        copy.wait_send()
    for copy in att_late + att_last:
        copy.wait_recv()
    for n in range(model // cols):
        total = product[:, columns(n)] + times(att_in[2], 3, n)
        total = total + times(att_in[0], 1, n) + times(att_in[1], 2, n)
        mixed_ref[:, columns(n)] = total.astype(BF16)


def body(tokens, query_weight, key_weight, value_weight, out_weight, query_gain, key_gain):
    rows, depth = tokens.shape
    query_cols = query_weight.shape[1]
    kv_cols = key_weight.shape[1]
    heads, width = query_gain.shape
    group, model = out_weight.shape
    count = rows * RING
    n_sp = RING * RING * 2
    n_tiles = 2 * heads * rows // TILE
    any_space = pl.BlockSpec(memory_space=pl.ANY)
    vmem = pl.BlockSpec(memory_space=pltpu.VMEM)
    dma = pltpu.SemaphoreType.DMA
    return pl.pallas_call(
        kernel,
        out_shape=(
            pltpu.VMEM((rows, model), BF16),
            pltpu.VMEM((heads, count), F32),
        ),
        in_specs=[any_space] * 5 + [vmem] * 2,
        out_specs=(vmem, vmem),
        scratch_shapes=[
            pltpu.VMEM((4, rows, depth), BF16),
            pltpu.VMEM((depth, query_cols), BF16),
            pltpu.VMEM((2 * kv_cols, depth), BF16),
            pltpu.VMEM((4, group, model), BF16),
            pltpu.VMEM((width, heads * rows + 128), F32),
            pltpu.VMEM((4, width, heads * rows), F32),
            pltpu.VMEM((2, 2, width, 2 * heads * rows), BF16),
            pltpu.VMEM((n_sp * count, 2 * width), BF16),
            pltpu.VMEM((2, 3, CHUNK, TILE), F32),
            pltpu.VMEM((2, 3, 8, TILE), F32),
            pltpu.VMEM((2, 2, width + ONES, CHUNK), BF16),
            pltpu.VMEM((2, 2, n_tiles, width + ONES, TILE), F32),
            pltpu.VMEM((2, 2, n_tiles, 1, TILE), F32),
            pltpu.VMEM((4, rows, group), BF16),
            pltpu.VMEM((3, rows, group), BF16),
            pltpu.VMEM((count, 128), F32),
            pltpu.VMEM((rows, model), F32),
            dma((5,)),
            dma((6,)),
            dma((4, 2)),
            dma((4,)),
            dma((4, RING, 2)),
            dma((12,)),
            dma((4, 4)),
            dma((5,)),
            dma((3, 2)),
        ],
        compiler_params=pltpu.CompilerParams(
            collective_id=0, has_side_effects=True, vmem_limit_bytes=60 * 1024 * 1024
        ),
        name="attention",
    )(tokens, query_weight, key_weight.T, value_weight.T, out_weight, query_gain, key_gain)


def solution(mesh):
    return jax.shard_map(
        body,
        mesh=mesh,
        in_specs=(
            P(("sp", "tp"), None),
            P(None, "tp"),
            P(None, "tp"),
            P(None, "tp"),
            P("tp", None),
            P("tp", None),
            P("tp", None),
        ),
        out_specs=(P(("sp", "tp"), None), P("tp", "sp")),
        check_vma=False,
    )
```

```python
import functools
import math

import jax
import jax.numpy as jnp
from jax import lax
from jax.experimental import pallas as pl
from jax.experimental.pallas import tpu as pltpu
from jax.sharding import PartitionSpec as P

GRID_W = 64
ROPE_BASE = 10000.0
EPS = 1e-06
LOG2E = math.log2(math.e)
LN2 = math.log(2.0)
ONES = 16
RING = 4
CHUNK = 768
TILE = 256
SUB = 256
MESH = pl.DeviceIdType.MESH
F32 = jnp.float32
BF16 = jnp.bfloat16


def prepare(x, gain, tables):
    quarter = x.shape[0] // 4
    x = x * lax.rsqrt(jnp.mean(x * x, axis=0, keepdims=True) + EPS) * gain
    a, b, c, d = (x[i * quarter : (i + 1) * quarter] for i in range(4))
    row_cos, row_sin, col_cos, col_sin = tables
    return jnp.concatenate(
        [
            a * row_cos - b * row_sin,
            b * row_cos + a * row_sin,
            c * col_cos - d * col_sin,
            d * col_cos + c * col_sin,
        ],
        axis=0,
    )


def kernel(
    tok_hbm,
    wq_hbm,
    wk_hbm,
    wv_hbm,
    wo_hbm,
    qg_ref,
    kg_ref,
    mixed_ref,
    log_ref,
    tok,
    wq,
    wkv,
    wo,
    gain_cols,
    tables,
    queries,
    kv,
    scores,
    peak,
    turned_v,
    acc,
    top,
    att,
    att_in,
    log_rows,
    product,
    local_sem,
    tok_send,
    tok_recv,
    kv_send,
    kv_recv,
    wo_send,
    wo_recv,
    att_send,
    att_recv,
):
    sp = lax.axis_index("sp")
    tp = lax.axis_index("tp")
    core = lax.rem(sp, 2)
    scores, peak, turned_v, acc, top, queries = (
        ref.at[core] for ref in (scores, peak, turned_v, acc, top, queries)
    )
    y = lax.rem(sp // 2, RING)
    z = sp // (2 * RING)
    mate = sp + 1 - 2 * core
    left, right, opposite = (lax.rem(tp + i, RING) for i in (3, 1, 2))
    rows = tok.shape[1]
    half = rows // 2
    heads, width = qg_ref.shape
    count = rows * RING
    kv_cols = wk_hbm.shape[0]
    group, model = wo_hbm.shape
    n_tiles = 2 * heads * rows // TILE

    coord_a = y * (1 - core) + z * core
    step_a = 2 + 6 * core
    coord_b = z * (1 - core) + y * core
    step_b = 8 - 6 * core

    def peer_a(i):
        return {"sp": sp + (lax.rem(coord_a + i, RING) - coord_a) * step_a}

    def peer_b(i):
        return {"sp": sp + (lax.rem(coord_b + i, RING) - coord_b) * step_b}

    loads = [
        pltpu.make_async_copy(src, dst, local_sem.at[i])
        for i, (src, dst) in enumerate(
            (
                (tok_hbm, tok.at[0]),
                (wk_hbm, wkv.at[0:kv_cols]),
                (wv_hbm, wkv.at[kv_cols:]),
                (wq_hbm, wq),
                (wo_hbm, wo.at[0]),
            )
        )
    ]
    for load in loads:
        load.start()

    barrier = pltpu.get_barrier_semaphore()
    for i in range(1, RING):
        pl.semaphore_signal(barrier, inc=1, device_id={"tp": lax.rem(tp + i, RING)}, device_id_type=MESH)
        pl.semaphore_signal(barrier, inc=1, device_id=peer_a(i), device_id_type=MESH)
        if i != 2:
            pl.semaphore_signal(barrier, inc=1, device_id=peer_b(i), device_id_type=MESH)
    pl.semaphore_signal(barrier, inc=1, device_id={"sp": mate}, device_id_type=MESH)
    pl.semaphore_wait(barrier, 3 * (RING - 1))

    def send(src, dst, send_sem, recv_sem, where):
        return pltpu.make_async_remote_copy(
            src_ref=src,
            dst_ref=dst,
            send_sem=send_sem,
            recv_sem=recv_sem,
            device_id=where,
            device_id_type=MESH,
        )

    def part(i):
        return slice(i * half, (i + 1) * half)

    to_left, to_right, to_opposite, to_mate = {"tp": left}, {"tp": right}, {"tp": opposite}, {"sp": mate}

    def token_copy(src, piece, i, slot, where):
        return send(src, tok.at[piece, part(i)], tok_send.at[slot], tok_recv.at[piece, i], where)

    first_half, second_half = tok_hbm.at[part(0)], tok_hbm.at[part(1)]
    token_out = [
        token_copy(first_half, 1, 0, 0, to_right),
        token_copy(second_half, 1, 1, 1, to_left),
        token_copy(second_half, 2, 0, 2, to_right),
        token_copy(first_half, 2, 1, 3, to_left),
    ]
    token_on = [
        token_copy(tok.at[1, part(0)], 3, 0, 4, to_right),
        token_copy(tok.at[1, part(1)], 3, 1, 5, to_left),
    ]
    for copy in token_out:
        copy.start()

    def token_wait(piece, i):
        token_copy(tok.at[1, part(i)], piece, i, 4 + i, to_right).wait_recv()

    starts = (
        (tp * rows, tp * rows + half),
        (left * rows, right * rows + half),
        (left * rows + half, right * rows),
        (opposite * rows, opposite * rows + half),
    )

    quarter = width // 4
    lane = lax.broadcasted_iota(jnp.int32, (quarter, heads * rows), 1)
    spot = lane
    for h in range(1, heads):
        spot = spot - jnp.where(lane >= h * rows, rows, 0)
    order = lax.broadcasted_iota(jnp.int32, (quarter, heads * rows), 0).astype(F32)
    freq = jnp.exp(order * (-math.log(ROPE_BASE) / quarter))
    shift = GRID_W.bit_length() - 1
    for p in range(4):
        a, b = starts[p]
        place = sp * count + spot + jnp.where(spot < half, a, b - half)
        row = lax.shift_right_logical(place, shift).astype(F32) * freq
        col = jnp.bitwise_and(place, GRID_W - 1).astype(F32) * freq
        tables[p, 0:quarter] = jnp.cos(row)
        tables[p, quarter : 2 * quarter] = jnp.sin(row)
        tables[p, 2 * quarter : 3 * quarter] = jnp.cos(col)
        tables[p, 3 * quarter :] = jnp.sin(col)

    gain_rows = [
        jnp.broadcast_to(qg_ref[h : h + 1, :].astype(F32) * (LOG2E * width ** (-0.5)), (rows, width))
        for h in range(heads)
    ]
    gain_rows.append(jnp.broadcast_to(kg_ref[...].astype(F32), (128, width)))
    gain_cols[...] = jnp.transpose(jnp.concatenate(gain_rows, axis=0))
    top[...] = jnp.full_like(top, -1e30)
    acc[...] = jnp.zeros_like(acc)
    turned_v[:, width:, :] = jnp.ones_like(turned_v[:, width:, :])
    log_rows[...] = jnp.zeros_like(log_rows)

    place_of = (0, 1, 3, 2)

    def kv_rows(p, shift, c, k, n):
        base = (((p * RING + place_of[shift]) * 2 + c) * RING + k) * rows
        return kv.at[pl.ds(pl.multiple_of(base, half), n)]

    def tables_of(p, n):
        return [tables[p, i * quarter : (i + 1) * quarter, 0:n] for i in range(4)]

    def make_kv(p):
        raw = lax.dot_general(tok[p], wkv[...], (((1,), (1,)), ((), ())), preferred_element_type=F32)
        turned = jnp.transpose(raw)
        gain = gain_cols[:, heads * rows : heads * rows + rows]
        keys = prepare(turned[0:width], gain, tables_of(p, rows))
        to = kv_rows(p, 0, core, 0, rows)
        to[:, 0:width] = jnp.transpose(keys).astype(BF16)
        to[:, width : 2 * width] = raw[:, width:].astype(BF16)

    def make_queries(p):
        raw = jnp.dot(tok[p], wq[...], preferred_element_type=F32)
        stacked = jnp.concatenate([raw[:, h * width : (h + 1) * width] for h in range(heads)], axis=0)
        q = prepare(jnp.transpose(stacked), gain_cols[:, 0 : heads * rows], tables_of(p, heads * rows))
        at = slice((p % 2) * heads * rows, (p % 2 + 1) * heads * rows)
        queries[p // 2, :, at] = q.astype(BF16)

    def kv_copy(src, dst, p, shift, c, where):
        return send(src, dst, kv_send.at[p], kv_recv.at[p, place_of[shift], c], where)

    whole = RING * rows

    def own_send(p):
        src = kv_rows(p, 0, core, 0, rows)
        for i in (1, 3, 2):
            kv_copy(src, kv_rows(p, 0, core, RING - i, rows), p, 0, core, peer_a(i)).start()

    def hand_copy(p, shift):
        spot = kv_rows(p, shift, core, 0, whole)
        return kv_copy(spot, spot, p, shift, core, to_mate)

    def spread(p):
        spot = kv_rows(p, 0, core, 1, whole - rows)
        kv_copy(spot, spot, p, 0, core, to_mate).wait_recv()
        src = kv_rows(p, 0, core, 0, whole)
        for i in (1, 3):
            kv_copy(src, kv_rows(p, RING - i, core, 0, whole), p, RING - i, core, peer_b(i)).start()
        hand_copy(p, 0).start()

    def relay(p):
        for shift, k, to in ((3, 0, 1), (1, 2, 3)):
            hand_copy(p, shift).wait_recv()
            src = kv_rows(p, shift, core, k, 2 * rows)
            kv_copy(src, kv_rows(p, 2, core, k, 2 * rows), p, 2, core, peer_b(to)).start()
            hand_copy(p, shift).start()

    def hand(p):
        hand_copy(p, 2).wait_recv()
        hand_copy(p, 2).start()

    def from_mate(p, shift):
        spot = kv_rows(p, shift, 1 - core, 0, whole)
        kv_copy(spot, spot, p, shift, 1 - core, to_mate).wait_recv()

    strip = group // 8
    parity = lax.rem(coord_a, 2)
    to_pair = {"sp": sp + (1 - 2 * parity) * step_a}

    def wo_rows(block, side, first, n):
        return wo.at[block, pl.ds(pl.multiple_of((side * 4 + first) * strip, strip), n * strip)]

    def wo_copy(block, to_block, i, slot, where):
        at = 2 * parity + i
        return send(
            wo_rows(block, core, at, 1), wo_rows(to_block, core, at, 1), wo_send.at[slot], wo_recv.at[to_block, i], where
        )

    wo_out = [
        wo_copy(0, 1, 0, 0, to_right),
        wo_copy(0, 2, 1, 1, to_left),
        wo_copy(0, 1, 1, 2, to_right),
        wo_copy(0, 2, 0, 3, to_left),
    ]
    wo_on = [wo_copy(1, 3, 0, 4, to_right), wo_copy(2, 3, 1, 5, to_left)]
    wo_rest = [wo_copy(0, 1, 1, 2, to_right), wo_copy(0, 2, 0, 3, to_left)]

    def pair_copy(block):
        spot = wo_rows(block, core, 2 * parity, 2)
        return send(spot, spot, wo_send.at[5 + block], wo_recv.at[block, 2], to_pair)

    def wo_hand(block, mine):
        spot = wo_rows(block, core, 2 * parity if mine else 2 - 2 * parity, 2)
        return send(spot, spot, wo_send.at[(8 if mine else 11) + block], wo_recv.at[block, 3], to_mate)

    def piece_work(p):
        make_kv(p)
        own_send(p)
        make_queries(p)

    loads[0].wait()
    loads[1].wait()
    loads[2].wait()
    make_kv(0)
    own_send(0)
    loads[3].wait()
    make_queries(0)
    spread(0)
    for i, copy in enumerate(token_on):
        token_wait(1, i)
        copy.start()
    loads[4].wait()
    for copy in wo_out:
        copy.start()
    piece_work(1)

    def turn(chunk, slot):
        at = pl.ds(pl.multiple_of(chunk * CHUNK, CHUNK), CHUNK)
        turned_v[slot, 0:width] = jnp.transpose(kv[at])[width : 2 * width]

    def score(chunk, side, t, slot, i):
        at = pl.ds(pl.multiple_of(chunk * CHUNK + i * SUB, SUB), SUB)
        q = queries[side, :, t * TILE : (t + 1) * TILE]
        s = jnp.dot(kv[at, 0:width], q, preferred_element_type=F32)
        scores[slot, i * SUB : (i + 1) * SUB] = s
        return jnp.max(s.reshape(SUB // 8, 8, TILE), axis=0)

    def score_all(chunk, side, t, slot):
        best = None
        for i in range(CHUNK // SUB):
            m = score(chunk, side, t, slot, i)
            best = m if best is None else jnp.maximum(best, m)
        peak[slot] = best

    def finish(side):
        flat = [acc[side, t] for t in range(n_tiles)]
        sums = jnp.concatenate([f[width : width + 8] for f in flat], axis=1)
        tops = jnp.concatenate([top[side, t] for t in range(n_tiles)], axis=1)
        outs = jnp.concatenate([f[0:width] / f[width : width + 1] for f in flat], axis=1)
        logs = (tops + jnp.log2(sums)) * LN2
        turned = jnp.transpose(jnp.concatenate([outs, logs], axis=0))
        for q in range(2):
            p = 2 * side + q
            for h in range(heads):
                base = (q * heads + h) * rows
                att[p, :, h * width : (h + 1) * width] = turned[base : base + rows, 0:width].astype(BF16)
        return turned

    def keep_logs(side, turned):
        for q in range(2):
            for h in range(heads):
                for i in range(2):
                    base = (q * heads + h) * rows + i * half
                    to = pl.ds(pl.multiple_of(starts[2 * side + q][i], half), half)
                    log_rows[to, h : h + 1] = turned[base : base + half, width : width + 1]

    def att_copy(p, i, source, at, slot, where):
        src = att.at[p] if i is None else att.at[p, part(i)]
        dst = att_in.at[source] if at is None else att_in.at[source, part(at)]
        return send(src, dst, att_send.at[slot], att_recv.at[source, at or 0], where)

    att_late = [
        att_copy(3, None, 2, None, 0, to_opposite),
        att_copy(2, 0, 1, 1, 1, to_left),
        att_copy(2, 1, 0, 0, 2, to_right),
    ]
    att_last = [att_copy(1, 0, 1, 0, 3, to_left), att_copy(1, 1, 0, 1, 4, to_right)]

    def wait_tokens(p):
        for i in range(2):
            token_wait(p, i)

    def wo_one():
        wo_copy(1, 1, 0, 4, to_right).wait_recv()
        wo_on[0].start()
        wo_copy(2, 2, 1, 5, to_left).wait_recv()
        wo_on[1].start()

    def wo_two():
        for copy, block in zip(wo_rest, (1, 2)):
            copy.wait_recv()
            pair_copy(block).start()
            wo_hand(block, True).start()

    def wo_three():
        for copy in wo_on:
            copy.wait_recv()
        pair_copy(3).start()
        wo_hand(3, True).start()

    def wo_swap(*blocks):
        for block in blocks:
            spot = wo_rows(block, core, 2 - 2 * parity, 2)
            send(spot, spot, wo_send.at[0], wo_recv.at[block, 2], to_pair).wait_recv()
            wo_hand(block, False).start()

    def close_late():
        keep_logs(1, finish(1))
        for copy in att_late:
            copy.start()

    def items(side, *spots):
        return [(p * RING + place_of[shift], side) for p, shift in spots]

    def both(*spots):
        return [item for spot in spots for item in items(1, spot) + items(0, spot)]

    def attend(item, after, slot_v):
        chunk, side = item
        for t in range(n_tiles):
            ahead = t + 2
            target = item if ahead < n_tiles else after
            if t == 1 and after is not None:
                turn(after[0], 1 - slot_v)
            tile, fill, slot = ahead % n_tiles, ahead % 3, t % 3
            old = top[side, t]
            new = jnp.maximum(old, jnp.max(peak[slot], axis=0, keepdims=True))
            best = None
            total = None
            for i in range(CHUNK // SUB):
                if target is not None:
                    m = score(target[0], target[1], tile, fill, i)
                    best = m if best is None else jnp.maximum(best, m)
                at = slice(i * SUB, (i + 1) * SUB)
                weights = jnp.exp2(scores[slot, at] - new).astype(BF16)
                mixed = jnp.dot(turned_v[slot_v, :, at], weights, preferred_element_type=F32)
                total = mixed if total is None else total + mixed
            if target is not None:
                peak[fill] = best
            acc[side, t] = acc[side, t] * jnp.exp2(old - new) + total
            top[side, t] = new

    def run(todo, slot_v, after=None, cold=False):
        if cold:
            turn(todo[0][0], slot_v)
            for t in range(2):
                score_all(todo[0][0], todo[0][1], t, t)
        for n, item in enumerate(todo):
            attend(item, todo[n + 1] if n + 1 < len(todo) else after, (slot_v + n) % 2)
        return (slot_v + len(todo)) % 2

    def next_piece(p):
        wait_tokens(p)
        piece_work(p)

    def mates(*spots):
        for spot in spots:
            from_mate(*spot)

    from_mate(0, 0)
    run(items(0, (0, 0)), 0, cold=True)
    relay(0)
    next_piece(2)
    spread(1)
    mates((0, 1), (0, 3))
    run(items(0, (0, 1), (0, 3)), 0, cold=True)
    hand(0)
    from_mate(1, 0)
    run(items(0, (1, 0)), 0, cold=True)
    next_piece(3)
    relay(1)
    spread(2)
    from_mate(0, 2)
    plan = [
        items(1, (0, 0), (0, 1), (0, 3)),
        both((0, 2)) + items(1, (1, 0)),
        both((1, 1)),
        both((1, 3)) + items(1, (2, 0)),
        items(0, (2, 0)) + both((1, 2)),
        both((2, 1)) + items(1, (2, 3)),
        items(0, (2, 3)) + both((3, 0)) + items(1, (3, 1)),
        items(0, (3, 1)) + items(1, (2, 2)),
        items(0, (2, 2)) + items(1, (3, 3)),
        items(1, (3, 2)),
        items(0, (3, 3), (3, 2)),
    ]

    def before(n):
        if n == 1:
            from_mate(1, 1)
        if n == 2:
            spread(3)
            hand(1)
            wo_one()
            mates((1, 3), (2, 0))
        if n == 3:
            relay(2)
            wo_two()
        if n == 4:
            mates((1, 2), (2, 1))
        if n == 5:
            relay(3)
            wo_three()
            from_mate(2, 3)
        if n == 6:
            hand(2)
            mates((3, 0), (3, 1))
        if n == 7:
            from_mate(2, 2)
        if n == 8:
            hand(3)
            from_mate(3, 3)
        if n == 9:
            from_mate(3, 2)
        if n == 10:
            close_late()
            wo_swap(1, 2)

    slot_v = 0
    for n, todo in enumerate(plan):
        before(n)
        ahead = plan[n + 1][0] if n + 1 < len(plan) and n != 8 else None
        slot_v = run(todo, slot_v, ahead, cold=n in (0, 9))

    turned = finish(0)
    for copy in att_last:
        copy.start()
    keep_logs(0, turned)
    log_ref[...] = jnp.transpose(log_rows[...])[0:heads]

    wo_swap(3)

    cols = 512

    def columns(n):
        return slice(n * cols, (n + 1) * cols)

    def times(x, block, n):
        return jnp.dot(x, wo[block, :, columns(n)], preferred_element_type=F32)

    for n in range(model // cols):
        product[:, columns(n)] = times(att[0], 0, n)
    for copy in token_out + token_on + wo_out + wo_on:
        copy.wait_send()
    for p in range(4):
        sent = kv.at[pl.ds(0, 31 * rows)]
        kv_copy(sent, sent, p, 0, core, to_mate).wait_send()
    for block in (1, 2, 3):
        pair_copy(block).wait_send()
        wo_hand(block, True).wait_send()
        wo_hand(block, False).wait_send()
        other = wo_rows(block, 1 - core, 0, 4)
        send(other, other, wo_send.at[0], wo_recv.at[block, 3], to_mate).wait_recv()
    for copy in att_late + att_last:
        copy.wait_send()
    for copy in att_late[1:] + att_last:
        copy.wait_recv()
    for n in range(model // cols):
        product[:, columns(n)] += times(att_in[0], 1, n) + times(att_in[1], 2, n)
    att_late[0].wait_recv()
    for n in range(model // cols):
        total = product[:, columns(n)] + times(att_in[2], 3, n)
        mixed_ref[:, columns(n)] = total.astype(BF16)


def body(tokens, query_weight, key_weight, value_weight, out_weight, query_gain, key_gain):
    rows, depth = tokens.shape
    query_cols = query_weight.shape[1]
    kv_cols = key_weight.shape[1]
    heads, width = query_gain.shape
    group, model = out_weight.shape
    count = rows * RING
    n_sp = RING * RING * 2
    n_tiles = 2 * heads * rows // TILE
    any_space = pl.BlockSpec(memory_space=pl.ANY)
    vmem = pl.BlockSpec(memory_space=pltpu.VMEM)
    dma = pltpu.SemaphoreType.DMA
    return pl.pallas_call(
        kernel,
        out_shape=(
            pltpu.VMEM((rows, model), BF16),
            pltpu.VMEM((heads, count), F32),
        ),
        in_specs=[any_space] * 5 + [vmem] * 2,
        out_specs=(vmem, vmem),
        scratch_shapes=[
            pltpu.VMEM((4, rows, depth), BF16),
            pltpu.VMEM((depth, query_cols), BF16),
            pltpu.VMEM((2 * kv_cols, depth), BF16),
            pltpu.VMEM((4, group, model), BF16),
            pltpu.VMEM((width, heads * rows + 128), F32),
            pltpu.VMEM((4, width, heads * rows), F32),
            pltpu.VMEM((2, 2, width, 2 * heads * rows), BF16),
            pltpu.VMEM((n_sp * count, 2 * width), BF16),
            pltpu.VMEM((2, 3, CHUNK, TILE), F32),
            pltpu.VMEM((2, 3, 8, TILE), F32),
            pltpu.VMEM((2, 2, width + ONES, CHUNK), BF16),
            pltpu.VMEM((2, 2, n_tiles, width + ONES, TILE), F32),
            pltpu.VMEM((2, 2, n_tiles, 1, TILE), F32),
            pltpu.VMEM((4, rows, group), BF16),
            pltpu.VMEM((3, rows, group), BF16),
            pltpu.VMEM((count, 128), F32),
            pltpu.VMEM((rows, model), F32),
            dma((5,)),
            dma((6,)),
            dma((4, 2)),
            dma((4,)),
            dma((4, RING, 2)),
            dma((15,)),
            dma((4, 4)),
            dma((5,)),
            dma((3, 2)),
        ],
        compiler_params=pltpu.CompilerParams(
            collective_id=0, has_side_effects=True, vmem_limit_bytes=60 * 1024 * 1024
        ),
        name="attention",
    )(tokens, query_weight, key_weight.T, value_weight.T, out_weight, query_gain, key_gain)


def solution(mesh):
    return jax.shard_map(
        body,
        mesh=mesh,
        in_specs=(
            P(("sp", "tp"), None),
            P(None, "tp"),
            P(None, "tp"),
            P(None, "tp"),
            P("tp", None),
            P("tp", None),
            P("tp", None),
        ),
        out_specs=(P(("sp", "tp"), None), P("tp", "sp")),
        check_vma=False,
    )
```
